32 devices in a mesh: sp: 8 (over z, x), tp: 4 (over y, core).
Axes of the slice: x: 2, y: 2, z: 4, core: 2. Of those that a mesh axis runs over, the one named last changes fastest.
Arguments:
- queries: bfloat16 [1024, 32, 128], P('sp', 'tp'), may hold values from -6 to 6
- keys: bfloat16 [1024, 8, 128], P('sp', 'tp'), may hold values from -6 to 6
- values: bfloat16 [1024, 8, 128], P('sp', 'tp'), may hold values from -6 to 6
- q_gain: float32 [128], replicated, may hold values from 0.2 to 8
- k_gain: float32 [128], replicated, may hold values from 0.2 to 8
- w_out: bfloat16 [4096, 2048], P('tp'), may hold values from -0.09375 to 0.09375
- residual: bfloat16 [1024, 2048], P(('sp', 'tp')), may hold values from -6 to 6
- gain_mix: float32 [2048], replicated, may hold values from 0.1 to 1.9
- gain_pre: float32 [2048], replicated, may hold values from 0.1 to 1.9
- routes: int32 [1024, 4], P(('sp', 'tp')), may hold values from 0 to 7, all different within a row; in each aligned block of 32 rows (0 to 31, 32 to 63, ...) at most 32 rows name the same one
- route_weights: float32 [1024, 4], P(('sp', 'tp')), may hold values from 0.1 to 1
- w_gate: bfloat16 [8, 2048, 2048], P('sp', None, 'tp'), may hold values from -0.5 to 0.5
- w_up: bfloat16 [8, 2048, 2048], P('sp', None, 'tp'), may hold values from -0.5 to 0.5
- w_down: bfloat16 [8, 2048, 2048], P('sp', 'tp'), may hold values from -0.125 to 0.125
- gain_moe: float32 [2048], replicated, may hold values from 0.1 to 1.9
Outputs:
- layer_out: bfloat16 [1024, 2048], P(('sp', 'tp'))
The draws below stay inside these ranges and needn't reach their ends.
Inputs may be any that keep to these rules, and one draw needn't show every extreme that they name: `routes`: each row names 4 different experts. In each aligned block of 32 rows (the rows of one device) no expert is named by more than 32 rows, a bound that some block reaches.
All inputs are finite; a program needn't handle non-finite values.
Results may differ from the reference program's by a relative error of at most 0.017.
The reference program's roundings to bfloat16 on the way count: a program that leaves them out, or rounds other values in their place, can miss the bound.
Values may be sent and summed in bfloat16 or wider, within the bound.
A program may use at most 128 MiB of HBM per device.

```python
import math
import jax
import jax.numpy as jnp
import numpy as np
from jax import lax

D = 2048
Q_HEADS = 32
KV_HEADS = 8
HD = 128
FF = 2048
TOP = 4
GRID_W = 64
TOKENS = 1024
TOK_TP = 32
EXPERTS = 8
CAP = 32
N_TP = 4


def gain_draw(key):
    return 1.0 + 0.18 * jax.random.truncated_normal(key, -4.0, 4.0, (HD,), jnp.float32)


def draw_q_gain(key, part):
    return gain_draw(jax.random.fold_in(key, 31))


def draw_k_gain(key, part):
    return gain_draw(jax.random.fold_in(key, 57))


def steps_of(own_key, shape, shards, least, high):
    def one(position, blocks):
        draws = jax.random.uniform(jax.random.fold_in(jax.random.fold_in(own_key, 6), position), (blocks,), jnp.float32, least / len(shards), high / len(shards))
        return jnp.repeat(jnp.exp(draws), shape[position] // blocks).reshape((-1,) + (1,) * (len(shape) - position - 1))

    loudness = one(*shards[0])
    for cut in shards[1:]:
        loudness = loudness * one(*cut)
    return loudness


def routed_block(stream_key, own, number, rows, number_of, top, bound, lean):
    order = jax.random.permutation(stream_key, number_of)
    packed, common = shares(number_of, rows * top, bound, lean, True), shares(number_of, rows * top, bound, lean, False)
    places = jnp.arange(number_of)

    def named(lengths, rotation):
        used = int((lengths > 0).sum())
        fixed = max(1, used // 4)
        shifted = fixed + (places - fixed + rotation * (used - fixed)) % max(1, number_of - fixed)
        return jnp.zeros((number_of,), jnp.int32).at[order[jnp.where(places < fixed, places, shifted)]].set(jnp.asarray(lengths, jnp.int32))

    lengths = jnp.where(number % 4 == 0, named(packed, number // 4), named(common, number - number // 4 - 1))
    mixed = jax.random.permutation(jax.random.fold_in(own, 3), number_of)
    donor, taker = mixed[0:number_of // 2 * 2:2], mixed[1:number_of // 2 * 2:2]
    room = jnp.minimum(lengths[donor] - 1, bound - lengths[taker]) // 2
    room = jnp.where((donor == order[0]) | (taker == order[0]) | (lengths[taker] == 0), 0, jnp.maximum(room, 0))
    shifted = jax.random.randint(jax.random.fold_in(own, 4), (number_of // 2,), 0, 1 << 20) % (room + 1)
    lengths = lengths.at[donor].add(-shifted).at[taker].add(shifted)
    members = jnp.searchsorted(jnp.cumsum(lengths), jnp.arange(rows * top), side="right").astype(jnp.int32)
    listing = members.reshape(top, rows).T
    listing = listing[jax.random.permutation(jax.random.fold_in(own, 1), rows)]
    rotation = jax.random.randint(jax.random.fold_in(own, 2), (rows, 1), 0, top)
    return jnp.take_along_axis(listing, (jnp.arange(top)[None, :] + rotation) % top, axis=1)


def shares(amount, total, limit, lean, full):
    portions = [(1 << 20) // math.isqrt(standing ** lean) + 1 for standing in range(1, amount + 1)]
    largest = limit if full else min(limit, max(-(-total // amount), total * portions[0] // sum(portions)))
    least = 1 if total - largest >= amount - 1 else 0
    given, spare = [largest] + [least] * (amount - 1), total - largest - least * (amount - 1)
    while spare > 0:
        free = [i for i in range(1, amount) if given[i] < largest] or [i for i in range(1, amount) if given[i] < limit]
        mass, remaining = sum([portions[i] for i in free]), spare
        for i in free:
            addition = min(limit - given[i], max(1, remaining * portions[i] // mass), spare)
            given[i] = given[i] + addition
            spare = spare - addition
    return np.array(given)


def normal_values(stream_key, dims, spread, limit, shards=(), kind=jnp.bfloat16):
    loudness = steps_of(stream_key, dims, shards, -0.22, 0.18) if shards else 1.0
    values = jax.random.normal(stream_key, dims, jnp.float32) * spread * loudness
    return jnp.minimum(jnp.maximum(values, -limit), limit).astype(kind)


def setup_inputs(seed: int = 0) -> dict:
    key_of = jax.random.split(jax.random.key(seed), 16)
    queries = normal_values(key_of[0], (TOKENS, Q_HEADS, HD), 1.0, 6.0, ((0, 8), (1, 4)))
    keys = normal_values(key_of[1], (TOKENS, KV_HEADS, HD), 1.0, 6.0, ((0, 8), (1, 4)))
    values = normal_values(key_of[2], (TOKENS, KV_HEADS, HD), 1.0, 6.0, ((0, 8), (1, 4)))
    q_gain = draw_q_gain(jax.random.fold_in(key_of[15], 71), 0)
    k_gain = draw_k_gain(jax.random.fold_in(key_of[15], 71), 0)
    w_out = normal_values(key_of[5], (Q_HEADS * HD, D), (Q_HEADS * HD) ** -0.5, 0.09375, ((0, 4),))
    residual = normal_values(key_of[6], (TOKENS, D), 1.0, 6.0, ((0, 32),))
    gain_mix = jnp.clip(1.0 + 0.18 * jax.random.normal(key_of[7], (D,), jnp.float32), 0.1, 1.9)
    gain_pre = jnp.clip(1.0 + 0.18 * jax.random.normal(key_of[8], (D,), jnp.float32), 0.1, 1.9)
    routes_keys = jax.random.split(jax.random.fold_in(key_of[9], 1), TOKENS // TOK_TP)
    routes_turns = jax.random.permutation(jax.random.fold_in(key_of[9], 3), TOKENS // TOK_TP)
    routes = jax.vmap(lambda own, number: routed_block(jax.random.fold_in(key_of[9], 2), own, number, TOK_TP, EXPERTS, TOP, CAP, 1))(routes_keys, routes_turns).reshape((TOKENS, TOP))
    route_weights = jnp.clip(jnp.exp(math.log(1.0) - 2.3025851 * jax.random.uniform(key_of[10], (TOKENS, TOP), jnp.float32) ** steps_of(key_of[10], (TOKENS, TOP), ((0, 32),), -0.2, 0.2)), 0.1, 1.0)
    w_gate = normal_values(key_of[11], (EXPERTS, D, FF), (D // 16) ** -0.5, 0.5, ((0, 8), (2, 4)))
    w_up = normal_values(key_of[12], (EXPERTS, D, FF), (D // 16) ** -0.5, 0.5, ((0, 8), (2, 4)))
    w_down = normal_values(key_of[13], (EXPERTS, FF, D), FF ** -0.5, 0.125, ((0, 8), (1, 4)))
    gain_moe = jnp.clip(1.0 + 0.18 * jax.random.normal(key_of[14], (D,), jnp.float32), 0.1, 1.9)
    return {"queries": queries, "keys": keys, "values": values, "q_gain": q_gain, "k_gain": k_gain, "w_out": w_out, "residual": residual, "gain_mix": gain_mix, "gain_pre": gain_pre, "routes": routes, "route_weights": route_weights, "w_gate": w_gate, "w_up": w_up, "w_down": w_down, "gain_moe": gain_moe}


norm_eps = 1e-06
rope_theta = 10000.0
clamp_limit = 7.0
swish_alpha = 1.702

def rope_tables(positions, head_size):
    row_index = (positions // GRID_W).astype(jnp.float32)
    col_index = (positions % GRID_W).astype(jnp.float32)
    freq_count = head_size // 4
    inverse = rope_theta ** (-jnp.arange(freq_count, dtype=jnp.float32) / freq_count)
    angles = jnp.stack([row_index[:, None] * inverse, col_index[:, None] * inverse], axis=1)
    return (jnp.cos(angles), jnp.sin(angles))

def turn(array_in, cosine_table, sine_table):
    token_count, head_count, head_size = array_in.shape
    split_field = array_in.reshape(token_count, head_count, 2, 2, head_size // 4)
    first_half = split_field[:, :, :, 0, :]
    second_half = split_field[:, :, :, 1, :]
    cos_wide = cosine_table[:, None]
    sin_wide = sine_table[:, None]
    turned = jnp.stack([first_half * cos_wide - second_half * sin_wide, second_half * cos_wide + first_half * sin_wide], axis=3)
    return turned.reshape(token_count, head_count, head_size)

def scale_rows(array_in, gain_vec):
    return array_in * lax.rsqrt(lax.optimization_barrier(jnp.mean(array_in * array_in, axis=-1, keepdims=True)) + norm_eps) * gain_vec

def reference(queries, keys, values, q_gain, k_gain, w_out, residual, gain_mix, gain_pre, routes, route_weights, w_gate, w_up, w_down, gain_moe):
    positions = jnp.arange(TOKENS, dtype=jnp.int32)
    cosine_table, sine_table = rope_tables(positions, HD)
    q_turned = (turn(scale_rows(queries.astype(jnp.float32), q_gain), cosine_table, sine_table) * HD ** (-0.5)).astype(jnp.bfloat16)
    k_turned = turn(scale_rows(keys.astype(jnp.float32), k_gain), cosine_table, sine_table).astype(jnp.bfloat16)
    group_size = Q_HEADS // KV_HEADS
    qblock = math.gcd(TOKENS, 512)
    blocks = q_turned.reshape(TOKENS // qblock, qblock, KV_HEADS, group_size, HD)
    k_wide = k_turned.astype(jnp.float32)
    v_wide = values.astype(jnp.float32)

    def attend(block):
        scores = jnp.einsum('qkgd,skd->kgqs', block.astype(jnp.float32), k_wide)
        unnorm = jnp.exp(scores - lax.optimization_barrier(jnp.max(scores, axis=-1, keepdims=True)))
        totals = lax.optimization_barrier(jnp.sum(unnorm, axis=-1))
        summed = jnp.einsum('kgqs,skd->qkgd', unnorm.astype(jnp.bfloat16).astype(jnp.float32), v_wide)
        return (summed / jnp.moveaxis(totals, 2, 0)[..., None]).astype(jnp.bfloat16)
    mixed_heads = lax.map(attend, blocks).reshape(TOKENS, Q_HEADS * HD)
    projected = jnp.dot(mixed_heads, w_out, preferred_element_type=jnp.float32)
    middle = residual.astype(jnp.float32) + scale_rows(projected, gain_mix)
    normed = scale_rows(middle, gain_pre).astype(jnp.bfloat16)
    block_count = TOKENS // TOK_TP
    assign = TOK_TP * TOP
    flat_routes = routes.reshape(block_count, assign)
    expert_hits = (flat_routes[:, :, None] == jnp.arange(EXPERTS, dtype=jnp.int32)[None, None, :]).astype(jnp.int32)
    slot_index = lax.optimization_barrier(jnp.sum((jnp.cumsum(expert_hits, axis=1) - expert_hits) * expert_hits, axis=2)).astype(jnp.int32)
    block_ids = jnp.broadcast_to(jnp.arange(block_count, dtype=jnp.int32)[:, None], (block_count, assign))
    token_ids = (block_ids * TOK_TP + jnp.arange(assign, dtype=jnp.int32)[None, :] // TOP).astype(jnp.int32)
    slot_tokens = jnp.full((EXPERTS, block_count, CAP), TOKENS, jnp.int32).at[flat_routes, block_ids, slot_index].set(token_ids)
    padded = jnp.concatenate([normed, jnp.zeros((1, D), jnp.bfloat16)], axis=0)
    group_width = FF // N_TP

    def serve_expert(expert_args):
        token_rows, gate_weight, up_weight, down_weight = expert_args
        arrived_rows = padded[token_rows.reshape(-1)]
        gate_pre = jnp.minimum(jnp.dot(arrived_rows, gate_weight, preferred_element_type=jnp.float32), clamp_limit)
        up_pre = jnp.clip(jnp.dot(arrived_rows, up_weight, preferred_element_type=jnp.float32), -clamp_limit, clamp_limit)
        active = (gate_pre * jax.nn.sigmoid(swish_alpha * gate_pre) * (up_pre + 1.0)).astype(jnp.bfloat16)
        group_sums = jnp.einsum('rqf,qfd->rqd', active.reshape(-1, N_TP, group_width).astype(jnp.float32), down_weight.reshape(N_TP, group_width, D).astype(jnp.float32))
        group_sums = lax.optimization_barrier(group_sums.astype(jnp.bfloat16)).astype(jnp.float32)
        return lax.optimization_barrier(jnp.sum(group_sums, axis=1)).astype(jnp.bfloat16)
    expert_out = lax.map(serve_expert, (slot_tokens, w_gate, w_up, w_down))
    picked = expert_out.reshape(EXPERTS, block_count, CAP, D)[flat_routes, block_ids, slot_index]
    picked = picked.reshape(TOKENS, TOP, D).astype(jnp.float32)
    mixture = lax.optimization_barrier(jnp.sum(picked * route_weights[:, :, None], axis=1))
    return (middle + scale_rows(mixture, gain_moe)).astype(jnp.bfloat16)
```

```python
import functools
import math
from types import SimpleNamespace

import jax
import jax.numpy as jnp
from jax import lax
from jax.experimental import pallas as pl
from jax.experimental.pallas import tpu as pltpu
from jax.sharding import PartitionSpec as P

TOP = 4
GRID_W = 64


norm_eps = 1e-06
rope_theta = 10000.0
clamp_limit = 7.0
swish_alpha = 1.702


def rope_tables(positions, head_size):
    row_index = (positions // GRID_W).astype(jnp.float32)
    col_index = (positions % GRID_W).astype(jnp.float32)
    freq_count = head_size // 4
    inverse = rope_theta ** (-jnp.arange(freq_count, dtype=jnp.float32) / freq_count)
    angles = jnp.stack([row_index[:, None] * inverse, col_index[:, None] * inverse], axis=1)
    return (jnp.cos(angles), jnp.sin(angles))


def turn(array_in, cosine_table, sine_table):
    token_count, head_count, head_size = array_in.shape
    split_field = array_in.reshape(token_count, head_count, 2, 2, head_size // 4)
    first_half = split_field[:, :, :, 0, :]
    second_half = split_field[:, :, :, 1, :]
    cos_wide = cosine_table[:, None]
    sin_wide = sine_table[:, None]
    turned = jnp.stack(
        [
            first_half * cos_wide - second_half * sin_wide,
            second_half * cos_wide + first_half * sin_wide,
        ],
        axis=3,
    )
    return turned.reshape(token_count, head_count, head_size)


def scale_rows(array_in, gain_vec):
    return (
        array_in
        * lax.rsqrt(jnp.mean(array_in * array_in, axis=-1, keepdims=True) + norm_eps)
        * gain_vec
    )


def slot_table(route_rows, experts, capacity):
    flat_routes = route_rows.reshape(-1)
    expert_hits = (flat_routes[:, None] == jnp.arange(experts, dtype=jnp.int32)[None, :]).astype(
        jnp.int32
    )
    slot_index = jnp.sum((jnp.cumsum(expert_hits, axis=0) - expert_hits) * expert_hits, axis=1)
    target = flat_routes * capacity + slot_index
    slot_onehot = target[:, None] == jnp.arange(experts * capacity, dtype=jnp.int32)[None, :]
    return slot_onehot.astype(jnp.bfloat16).reshape(
        route_rows.shape[0], route_rows.shape[1], experts * capacity
    )


def expert_apply(arrived_rows, w_gate, w_up, w_down):
    gate_pre = jnp.minimum(
        jnp.einsum("serd,edf->serf", arrived_rows, w_gate, preferred_element_type=jnp.float32),
        clamp_limit,
    )
    up_pre = jnp.clip(
        jnp.einsum("serd,edf->serf", arrived_rows, w_up, preferred_element_type=jnp.float32),
        -clamp_limit,
        clamp_limit,
    )
    active = (gate_pre * jax.nn.sigmoid(swish_alpha * gate_pre) * (up_pre + 1.0)).astype(
        jnp.bfloat16
    )
    partial_value = jnp.einsum("serf,efd->serd", active, w_down, preferred_element_type=jnp.float32)
    return lax.optimization_barrier(partial_value.astype(jnp.bfloat16)).astype(jnp.float32)


def send_back(finished):
    return lax.all_to_all(finished, "sp", split_axis=0, concat_axis=0, tiled=True)


MESH = pl.DeviceIdType.MESH
RING = 4
PAIR = 2
LANES = 128


def gather_kernel(n, own_ref, out_ref, send_sem, recv_sem, pass_sem, take_sem, own_sem):
    me = lax.axis_index("sp")
    tp = lax.axis_index("tp")
    pair = me + 1 - 2 * lax.rem(me, 2)
    barrier = pltpu.get_barrier_semaphore()

    def greet(i, carry):
        pl.semaphore_signal(
            barrier, inc=1, device_id=(lax.rem(me + 2 * i, n), tp), device_id_type=MESH
        )
        return carry

    lax.fori_loop(1, n // 2, greet, 0)
    pl.semaphore_signal(barrier, inc=1, device_id=(pair, tp), device_id_type=MESH)
    keep = pltpu.make_async_copy(own_ref, out_ref.at[me], own_sem)
    keep.start()
    pl.semaphore_wait(barrier, n // 2)

    def along(i):
        return pltpu.make_async_remote_copy(
            src_ref=own_ref,
            dst_ref=out_ref.at[me],
            send_sem=send_sem.at[i],
            recv_sem=recv_sem.at[i],
            device_id=(lax.rem(me + 2 * i, n), tp),
            device_id_type=MESH,
        )

    def across(i, src):
        return pltpu.make_async_remote_copy(
            src_ref=src,
            dst_ref=out_ref.at[lax.rem(me + n - 2 * i, n)],
            send_sem=pass_sem.at[i],
            recv_sem=take_sem.at[i],
            device_id=(pair, tp),
            device_id_type=MESH,
        )

    def relay(i):
        return across(i, out_ref.at[lax.rem(me + n - 2 * i, n)])

    def start(i, carry):
        along(i).start()
        return carry

    def forward(i, carry):
        along(i).wait_recv()
        relay(i).start()
        return carry

    def finish(i, carry):
        along(i).wait_send()
        relay(i).wait()
        return carry

    lax.fori_loop(1, n // 2, start, 0)
    across(0, own_ref).start()
    keep.wait()
    lax.fori_loop(1, n // 2, forward, 0)
    across(0, own_ref).wait()
    lax.fori_loop(1, n // 2, finish, 0)


def gather_sp(block):
    n = lax.axis_size("sp")
    return pl.pallas_call(
        functools.partial(gather_kernel, n),
        out_shape=jax.ShapeDtypeStruct((n,) + block.shape, block.dtype),
        in_specs=[pl.BlockSpec(memory_space=pltpu.VMEM)],
        out_specs=pl.BlockSpec(memory_space=pltpu.VMEM),
        scratch_shapes=[
            pltpu.SemaphoreType.DMA((n // 2,)),
            pltpu.SemaphoreType.DMA((n // 2,)),
            pltpu.SemaphoreType.DMA((n // 2,)),
            pltpu.SemaphoreType.DMA((n // 2,)),
            pltpu.SemaphoreType.DMA,
        ],
        compiler_params=pltpu.CompilerParams(collective_id=0, has_side_effects=True),
        cost_estimate=pl.CostEstimate(flops=0, bytes_accessed=1 << 24, transcendentals=0),
        name="gather_kv",
    )(block)


def wide(value):
    return value.astype(jnp.float32)


def experts_kernel(names, *refs):
    r = SimpleNamespace(**dict(zip(names, refs)))
    sp = lax.axis_index("sp")
    tp = lax.axis_index("tp")
    z, x = sp // PAIR, lax.rem(sp, PAIR)
    y, c = tp // PAIR, lax.rem(tp, PAIR)
    ox, oy, oc = 1 - x, 1 - y, 1 - c
    width = r.residual.shape[1]
    half = r.residual.shape[0] // 2
    top, bottom = pl.ds(0, half), pl.ds(half, half)
    upper = z // 2
    folded = z + upper * (RING - 1 - 2 * z)

    def plane(o):
        return o + upper * (RING - 1 - 2 * o)

    groups = (z, plane(folded + 1), plane(2 - 2 * folded), plane(RING - 1))
    to_c = (sp, y * PAIR + oc)
    to_y = (sp, oy * PAIR + c)
    to_x = (z * PAIR + ox, tp)
    to_z = [None] + [(g * PAIR + x, tp) for g in groups[1:]]
    peers = [to_c, to_y, to_x] + to_z[1:]
    mine, xb, yb, db = x * PAIR + y, ox * PAIR + y, x * PAIR + oy, ox * PAIR + oy

    loads = [
        pltpu.make_async_copy(a, b, r.w_sem.at[i])
        for i, (a, b) in enumerate(((r.wg_hbm, r.wg), (r.wu_hbm, r.wu), (r.wd_hbm, r.wd)))
    ]
    for load in loads:
        load.start()
    barrier = pltpu.get_barrier_semaphore()
    for peer in peers:
        pl.semaphore_signal(barrier, inc=1, device_id=peer, device_id_type=MESH)
    pl.semaphore_wait(barrier, len(peers))

    started = []

    def send(src, dst, s, t, to):
        copy = pltpu.make_async_remote_copy(
            src_ref=src, dst_ref=dst, send_sem=s, recv_sem=t, device_id=to, device_id_type=MESH
        )
        copy.start()
        started.append(copy)
        return copy

    def narrow(value):
        return value.astype(jnp.bfloat16)

    with jax.named_scope("proj"):
        first = send(r.part.at[oy, oc], r.pc_in.at[0], r.pc_s.at[0], r.pc_r.at[0], to_c)
        second = send(r.part.at[y, oc], r.pc_in.at[1], r.pc_s.at[1], r.pc_r.at[1], to_c)
        first.wait_recv()
        r.py_out[...] = narrow(wide(r.part[oy, c]) + wide(r.pc_in[0]))
        third = send(r.py_out, r.py_in, r.py_s.at[0], r.py_r.at[0], to_y)
        second.wait_recv()
        projected = wide(r.part[y, c]) + wide(r.pc_in[1])
        third.wait_recv()
        projected = projected + wide(r.py_in[...])
        mid = wide(r.residual[...]) + scale_rows(projected, r.gain_mix[...])
        r.middle[...] = mid
        r.got[z, c, mine, :, 0:width] = narrow(scale_rows(mid, r.gain_pre[...]))
        r.got[z, c, mine, :, width:] = r.tail[...]

    def block(p, k, rows=slice(None)):
        return r.got.at[groups[p], c, k, rows]

    z_copy, x_copy, y_copy = [None] * 4, [None] * 4, [None] * 4
    hx_copy, hy_copy = [None] * 4, [None] * 4
    relays = [[] for _ in range(4)]

    def relay(p, k, slot):
        relays[p].append(
            send(block(p, k), block(p, k), r.c_s.at[p, slot], r.c_r.at[p, slot], to_c)
        )

    def spread(p):
        if p:
            pltpu.make_async_remote_copy(
                src_ref=block(p, mine), dst_ref=block(p, mine), send_sem=r.z_s.at[p],
                recv_sem=r.z_r.at[groups[p]], device_id=to_z[p], device_id_type=MESH,
            ).wait_recv()
        x_copy[p] = send(block(p, mine), block(p, mine), r.x_s.at[p], r.x_r.at[p], to_x)
        y_copy[p] = send(block(p, mine), block(p, mine), r.y_s.at[p], r.y_r.at[p], to_y)
        relay(p, mine, 0)

    def cross(p):
        x_copy[p].wait_recv()
        hy_copy[p] = send(
            block(p, xb, top), block(p, xb, top), r.hy_s.at[p], r.hy_r.at[p], to_y
        )
        relay(p, xb, 1)
        y_copy[p].wait_recv()
        hx_copy[p] = send(
            block(p, yb, bottom), block(p, yb, bottom), r.hx_s.at[p], r.hx_r.at[p], to_x
        )
        relay(p, yb, 2)

    def corner(p):
        hx_copy[p].wait_recv()
        hy_copy[p].wait_recv()
        relay(p, db, 3)

    per = r.got.shape[2] * r.got.shape[3]

    def serve(p):
        for copy in relays[p]:
            copy.wait_recv()
        g = groups[p]
        spread_w = wide(r.got[g, :, :, :, width:].reshape(2 * per, LANES))
        lane = lax.broadcasted_iota(jnp.int32, spread_w.shape, 1)
        chosen = lax.rem(lane, LANES // 2) == sp
        coef = jnp.sum(jnp.where(chosen, spread_w, 0.0), axis=1, keepdims=True)
        step = min(r.wg.shape[1], 256)

        @pl.loop(0, r.wg.shape[1] // step)
        def _(i):
            cols = pl.ds(pl.multiple_of(i * step, step), step)
            rows = r.got[g, :, :, :, 0:width].reshape(2 * per, width)
            gate = jnp.dot(rows, r.wg[:, cols], preferred_element_type=jnp.float32)
            up = jnp.dot(rows, r.wu[:, cols], preferred_element_type=jnp.float32)
            gate = jnp.minimum(gate, clamp_limit)
            up = jnp.clip(up, -clamp_limit, clamp_limit)
            r.active[:, cols] = narrow(gate * jax.nn.sigmoid(swish_alpha * gate) * (up + 1.0))

        @pl.loop(0, width // 512)
        def _(i):
            cols = pl.ds(pl.multiple_of(i * 512, 512), 512)
            down = jnp.dot(r.active[...], r.wd[:, cols], preferred_element_type=jnp.float32)
            r.partial[p, :, :, :, cols] = narrow(down * coef).reshape(
                r.partial.shape[1:4] + (512,)
            )

        back[p] = send(r.partial.at[p, oc], r.core_in.at[p], r.rc_s.at[p], r.rc_r.at[p], to_c)

    back = [None] * 4
    dx_copy, dy_copy = [None] * 4, [None] * 4
    bx_copy, by_copy = [[] for _ in range(4)], [[] for _ in range(4)]
    home = [None] * 4

    def give_x(p, i, rows):
        bx_copy[p].append(
            send(
                r.summed.at[p, xb, rows], r.x_in.at[p, rows],
                r.bx_s.at[p, i], r.bx_r.at[p, i], to_x,
            )
        )

    def give_y(p, i, rows):
        by_copy[p].append(
            send(
                r.summed.at[p, yb, rows], r.y_in.at[p, rows],
                r.by_s.at[p, i], r.by_r.at[p, i], to_y,
            )
        )

    def fold(p):
        back[p].wait_recv()
        for k in (db, xb, yb, mine):
            r.summed[p, k] = narrow(wide(r.partial[p, c, k]) + wide(r.core_in[p, k]))
        dx_copy[p] = send(
            r.summed.at[p, db, top], r.dx_in.at[p], r.dx_s.at[p], r.dx_r.at[p], to_x
        )
        dy_copy[p] = send(
            r.summed.at[p, db, bottom], r.dy_in.at[p], r.dy_s.at[p], r.dy_r.at[p], to_y
        )
        give_x(p, 0, top)
        give_y(p, 0, bottom)

    def join(p):
        dx_copy[p].wait_recv()
        r.summed[p, yb, top] = narrow(wide(r.summed[p, yb, top]) + wide(r.dx_in[p]))
        give_y(p, 1, top)
        dy_copy[p].wait_recv()
        r.summed[p, xb, bottom] = narrow(wide(r.summed[p, xb, bottom]) + wide(r.dy_in[p]))
        give_x(p, 1, bottom)

    def gather(p):
        for copy in bx_copy[p] + by_copy[p]:
            copy.wait_recv()
        return wide(r.summed[p, mine]) + wide(r.x_in[p]) + wide(r.y_in[p])

    def leave(p):
        r.home_out[p] = narrow(gather(p))
        home[p] = send(
            r.home_out.at[p], r.home_in.at[z], r.b_s.at[p], r.b_r.at[z], to_z[p]
        )

    with jax.named_scope("spread"):
        for p in range(1, 4):
            z_copy[p] = send(block(0, mine), block(0, mine), r.z_s.at[p], r.z_r.at[z], to_z[p])
        spread(0)
        cross(0)
        spread(1)
        corner(0)
    for load in loads:
        load.wait()
    with jax.named_scope("serve"):
        cross(1)
        spread(2)
        serve(0)
        corner(1)
        cross(2)
        spread(3)
        fold(0)
        serve(1)
        join(0)
        corner(2)
        cross(3)
        fold(1)
        serve(2)
        join(1)
        corner(3)
        fold(2)
        serve(3)
        leave(1)
        join(2)
        fold(3)
        leave(2)
        join(3)
        mixture = gather(0)
        leave(3)
    with jax.named_scope("back"):
        for p in range(1, 4):
            g = groups[p]
            pltpu.make_async_remote_copy(
                src_ref=r.home_out.at[p], dst_ref=r.home_in.at[g], send_sem=r.b_s.at[p],
                recv_sem=r.b_r.at[g], device_id=to_z[p], device_id_type=MESH,
            ).wait_recv()
            mixture = mixture + wide(r.home_in[g])
        r.out[...] = (r.middle[...] + scale_rows(mixture, r.gain_moe[...])).astype(r.out.dtype)
        for copy in started:
            copy.wait_send()


def experts_layer(part, residual, gain_mix, gain_pre, gain_moe, tail, w_gate, w_up, w_down):
    tok, width = residual.shape
    ff = w_gate.shape[1]
    full = width + tail.shape[1]
    blocks = PAIR * PAIR
    half = tok // 2
    bf, f32 = jnp.bfloat16, jnp.float32
    dma = pltpu.SemaphoreType.DMA
    here = pl.BlockSpec(memory_space=pltpu.VMEM)
    there = pl.BlockSpec(memory_space=pl.ANY)
    scratch = {
        "wg": pltpu.VMEM((width, ff), bf),
        "wu": pltpu.VMEM((width, ff), bf),
        "wd": pltpu.VMEM((ff, width), bf),
        "pc_in": pltpu.VMEM((PAIR, tok, width), bf),
        "py_out": pltpu.VMEM((tok, width), bf),
        "py_in": pltpu.VMEM((tok, width), bf),
        "got": pltpu.VMEM((RING, PAIR, blocks, tok, full), bf),
        "middle": pltpu.VMEM((tok, width), f32),
        "active": pltpu.VMEM((PAIR * blocks * tok, ff), bf),
        "partial": pltpu.VMEM((RING, PAIR, blocks, tok, width), bf),
        "core_in": pltpu.VMEM((RING, blocks, tok, width), bf),
        "summed": pltpu.VMEM((RING, blocks, tok, width), bf),
        "dx_in": pltpu.VMEM((RING, half, width), bf),
        "dy_in": pltpu.VMEM((RING, half, width), bf),
        "x_in": pltpu.VMEM((RING, tok, width), bf),
        "y_in": pltpu.VMEM((RING, tok, width), bf),
        "home_out": pltpu.VMEM((RING, tok, width), bf),
        "home_in": pltpu.VMEM((RING, tok, width), bf),
        "w_sem": dma((3,)),
    }
    for name, dims in (
        ("pc", (2,)), ("py", (1,)), ("z", (4,)), ("x", (4,)), ("y", (4,)), ("hx", (4,)),
        ("hy", (4,)), ("c", (4, 4)), ("rc", (4,)), ("dx", (4,)), ("dy", (4,)), ("bx", (4, 2)),
        ("by", (4, 2)), ("b", (4,)),
    ):
        scratch[name + "_s"] = dma(dims)
        scratch[name + "_r"] = dma(dims)
    operands = (
        "part", "residual", "gain_mix", "gain_pre", "gain_moe", "tail", "wg_hbm", "wu_hbm",
        "wd_hbm",
    )
    names = operands + ("out",) + tuple(scratch)
    return pl.pallas_call(
        functools.partial(experts_kernel, names),
        out_shape=jax.ShapeDtypeStruct((tok, width), bf),
        in_specs=[here] * 6 + [there] * 3,
        out_specs=here,
        scratch_shapes=list(scratch.values()),
        compiler_params=pltpu.CompilerParams(
            collective_id=1, has_side_effects=True, vmem_limit_bytes=56 << 20
        ),
        name="experts_layer",
    )(part, residual, gain_mix, gain_pre, gain_moe, tail, w_gate, w_up, w_down)


def weight_tail(routes, route_weights, experts):
    hits = routes[:, :, None] == jnp.arange(experts, dtype=jnp.int32)[None, None, :]
    coef = jnp.sum(jnp.where(hits, route_weights[:, :, None], 0.0), axis=1)
    high = lax.reduce_precision(coef, 8, 7)
    low = coef - high
    gap = jnp.zeros((coef.shape[0], LANES // 2 - experts), jnp.float32)
    return jnp.concatenate([high, gap, low, gap], axis=1).astype(jnp.bfloat16)


def on_device(
    queries,
    keys,
    values,
    q_gain,
    k_gain,
    w_out,
    residual,
    gain_mix,
    gain_pre,
    routes,
    route_weights,
    w_gate,
    w_up,
    w_down,
    gain_moe,
):
    tok_rows, head_local, head_size = queries.shape
    kv_local = keys.shape[1]
    group_size = head_local // kv_local
    positions = lax.axis_index("sp") * tok_rows + jnp.arange(tok_rows, dtype=jnp.int32)
    cosine_table, sine_table = rope_tables(positions, head_size)
    q_turned = (
        turn(scale_rows(queries.astype(jnp.float32), q_gain), cosine_table, sine_table)
        * head_size ** (-0.5)
    ).astype(jnp.bfloat16)
    k_turned = turn(scale_rows(keys.astype(jnp.float32), k_gain), cosine_table, sine_table).astype(
        jnp.bfloat16
    )
    q_grouped = q_turned.reshape(tok_rows, kv_local, group_size, head_size)
    initial = (
        jnp.full((kv_local, group_size, tok_rows), -jnp.inf, jnp.float32),
        jnp.zeros((kv_local, group_size, tok_rows), jnp.float32),
        jnp.zeros((kv_local, group_size, tok_rows, head_size), jnp.float32),
    )
    carry_state = initial
    kv_cols = kv_local * head_size
    both = gather_sp(
        jnp.concatenate(
            [k_turned.reshape(tok_rows, kv_cols), values.reshape(tok_rows, kv_cols)], axis=1
        )
    ).reshape(-1, 2 * kv_cols)
    key_piece = both[:, :kv_cols].reshape(-1, kv_local, head_size)
    value_piece = both[:, kv_cols:].reshape(-1, kv_local, head_size)
    piece_rows = key_piece.shape[0]
    block_rows = math.gcd(piece_rows, 1024)
    key_blocks = key_piece.reshape(piece_rows // block_rows, block_rows, kv_local, head_size)
    value_blocks = value_piece.reshape(piece_rows // block_rows, block_rows, kv_local, head_size)

    def absorb_block(state_now, key_value):
        running_max, running_sum, weighted = state_now
        key_block, value_block = key_value
        scores = jnp.einsum(
            "qkgd,skd->kgqs", q_grouped, key_block, preferred_element_type=jnp.float32
        )
        new_max = jnp.maximum(running_max, jnp.max(scores, axis=-1))
        rescale = jnp.exp(running_max - new_max)
        unnorm = jnp.exp(scores - new_max[..., None])
        running_sum = running_sum * rescale + jnp.sum(unnorm, axis=-1)
        weighted = weighted * rescale[..., None] + jnp.einsum(
            "kgqs,skd->kgqd",
            unnorm.astype(jnp.bfloat16),
            value_block,
            preferred_element_type=jnp.float32,
        )
        return ((new_max, running_sum, weighted), None)

    carry_state, ignored = lax.scan(absorb_block, carry_state, (key_blocks, value_blocks))
    running_max, running_sum, weighted = carry_state
    mixed_heads = (weighted / running_sum[..., None]).transpose(2, 0, 1, 3)
    mixed_heads = mixed_heads.reshape(tok_rows, head_local * head_size).astype(jnp.bfloat16)
    tok_part = residual.shape[0]
    width = residual.shape[1]
    part = jnp.dot(mixed_heads, w_out, preferred_element_type=jnp.float32).astype(jnp.bfloat16)
    local_experts = w_gate.shape[0]
    experts_all = local_experts * lax.axis_size("sp")
    capacity = max(2, (2 * tok_part * TOP + experts_all - 1) // experts_all)
    grid_fits = lax.axis_size("sp") == RING * PAIR and lax.axis_size("tp") == PAIR * PAIR
    if grid_fits and local_experts == 1 and capacity >= tok_part:
        return experts_layer(
            part.reshape(PAIR, PAIR, tok_part, width),
            residual,
            gain_mix[None],
            gain_pre[None],
            gain_moe[None],
            weight_tail(routes, route_weights, experts_all),
            w_gate[0],
            w_up[0],
            w_down[0],
        )
    projected = lax.psum_scatter(
        part,
        "tp",
        scatter_dimension=0,
        tiled=True,
    ).astype(jnp.float32)
    middle = residual.astype(jnp.float32) + scale_rows(projected, gain_mix)
    normed = scale_rows(middle, gain_pre).astype(jnp.bfloat16)
    tables = slot_table(routes, experts_all, capacity)
    chosen = jnp.sum(tables, axis=1)
    outbound = jnp.einsum("tp,td->pd", chosen, normed, preferred_element_type=jnp.float32)
    outbound = outbound.astype(jnp.bfloat16).reshape(experts_all, capacity, width)
    arrived_rows = lax.all_gather(
        lax.all_to_all(outbound, "sp", split_axis=0, concat_axis=0, tiled=True),
        "tp",
        axis=0,
        tiled=True,
    )
    leading = arrived_rows.shape[0] // local_experts
    partial_value = expert_apply(
        arrived_rows.reshape(leading, local_experts, arrived_rows.shape[1], width),
        w_gate,
        w_up,
        w_down,
    )
    summed = lax.psum_scatter(
        partial_value.reshape(arrived_rows.shape).astype(jnp.bfloat16),
        "tp",
        scatter_dimension=0,
        tiled=True,
    )
    returned = send_back(summed)
    gathered = jnp.einsum(
        "tkp,pd->tkd",
        tables,
        returned.reshape(experts_all * capacity, width),
        preferred_element_type=jnp.float32,
    )
    mixture = jnp.sum(gathered * route_weights[:, :, None], axis=1)
    return (middle + scale_rows(mixture, gain_moe)).astype(jnp.bfloat16)


def solution(mesh):
    placed = (
        P("sp", "tp", None),
        P("sp", "tp", None),
        P("sp", "tp", None),
        P(),
        P(),
        P("tp", None),
        P(("sp", "tp"), None),
        P(),
        P(),
        P(("sp", "tp"), None),
        P(("sp", "tp"), None),
        P("sp", None, "tp"),
        P("sp", None, "tp"),
        P("sp", "tp", None),
        P(),
    )
    return jax.shard_map(
        on_device, mesh=mesh, in_specs=placed, out_specs=P(("sp", "tp"), None), check_vma=False
    )
```

```python
import functools
import math
from types import SimpleNamespace

import jax
import jax.numpy as jnp
from jax import lax
from jax.experimental import pallas as pl
from jax.experimental.pallas import tpu as pltpu
from jax.sharding import PartitionSpec as P

TOP = 4
GRID_W = 64


norm_eps = 1e-06
rope_theta = 10000.0
clamp_limit = 7.0
swish_alpha = 1.702


def rope_tables(positions, head_size):
    row_index = (positions // GRID_W).astype(jnp.float32)
    col_index = (positions % GRID_W).astype(jnp.float32)
    freq_count = head_size // 4
    inverse = rope_theta ** (-jnp.arange(freq_count, dtype=jnp.float32) / freq_count)
    angles = jnp.stack([row_index[:, None] * inverse, col_index[:, None] * inverse], axis=1)
    return (jnp.cos(angles), jnp.sin(angles))


def turn(array_in, cosine_table, sine_table):
    token_count, head_count, head_size = array_in.shape
    split_field = array_in.reshape(token_count, head_count, 2, 2, head_size // 4)
    first_half = split_field[:, :, :, 0, :]
    second_half = split_field[:, :, :, 1, :]
    cos_wide = cosine_table[:, None]
    sin_wide = sine_table[:, None]
    turned = jnp.stack(
        [
            first_half * cos_wide - second_half * sin_wide,
            second_half * cos_wide + first_half * sin_wide,
        ],
        axis=3,
    )
    return turned.reshape(token_count, head_count, head_size)


def scale_rows(array_in, gain_vec):
    return (
        array_in
        * lax.rsqrt(jnp.mean(array_in * array_in, axis=-1, keepdims=True) + norm_eps)
        * gain_vec
    )


def slot_table(route_rows, experts, capacity):
    flat_routes = route_rows.reshape(-1)
    expert_hits = (flat_routes[:, None] == jnp.arange(experts, dtype=jnp.int32)[None, :]).astype(
        jnp.int32
    )
    slot_index = jnp.sum((jnp.cumsum(expert_hits, axis=0) - expert_hits) * expert_hits, axis=1)
    target = flat_routes * capacity + slot_index
    slot_onehot = target[:, None] == jnp.arange(experts * capacity, dtype=jnp.int32)[None, :]
    return slot_onehot.astype(jnp.bfloat16).reshape(
        route_rows.shape[0], route_rows.shape[1], experts * capacity
    )


def expert_apply(arrived_rows, w_gate, w_up, w_down):
    gate_pre = jnp.minimum(
        jnp.einsum("serd,edf->serf", arrived_rows, w_gate, preferred_element_type=jnp.float32),
        clamp_limit,
    )
    up_pre = jnp.clip(
        jnp.einsum("serd,edf->serf", arrived_rows, w_up, preferred_element_type=jnp.float32),
        -clamp_limit,
        clamp_limit,
    )
    active = (gate_pre * jax.nn.sigmoid(swish_alpha * gate_pre) * (up_pre + 1.0)).astype(
        jnp.bfloat16
    )
    partial_value = jnp.einsum("serf,efd->serd", active, w_down, preferred_element_type=jnp.float32)
    return lax.optimization_barrier(partial_value.astype(jnp.bfloat16)).astype(jnp.float32)


def send_back(finished):
    return lax.all_to_all(finished, "sp", split_axis=0, concat_axis=0, tiled=True)


MESH = pl.DeviceIdType.MESH
RING = 4
PAIR = 2
LANES = 128


def gather_kernel(n, own_ref, out_ref, send_sem, recv_sem, pass_sem, take_sem, own_sem):
    me = lax.axis_index("sp")
    tp = lax.axis_index("tp")
    pair = me + 1 - 2 * lax.rem(me, 2)
    barrier = pltpu.get_barrier_semaphore()

    def greet(i, carry):
        pl.semaphore_signal(
            barrier, inc=1, device_id=(lax.rem(me + 2 * i, n), tp), device_id_type=MESH
        )
        return carry

    lax.fori_loop(1, n // 2, greet, 0)
    pl.semaphore_signal(barrier, inc=1, device_id=(pair, tp), device_id_type=MESH)
    keep = pltpu.make_async_copy(own_ref, out_ref.at[me], own_sem)
    keep.start()
    pl.semaphore_wait(barrier, n // 2)

    def along(i):
        return pltpu.make_async_remote_copy(
            src_ref=own_ref,
            dst_ref=out_ref.at[me],
            send_sem=send_sem.at[i],
            recv_sem=recv_sem.at[i],
            device_id=(lax.rem(me + 2 * i, n), tp),
            device_id_type=MESH,
        )

    def across(i, src):
        return pltpu.make_async_remote_copy(
            src_ref=src,
            dst_ref=out_ref.at[lax.rem(me + n - 2 * i, n)],
            send_sem=pass_sem.at[i],
            recv_sem=take_sem.at[i],
            device_id=(pair, tp),
            device_id_type=MESH,
        )

    def relay(i):
        return across(i, out_ref.at[lax.rem(me + n - 2 * i, n)])

    def start(i, carry):
        along(i).start()
        return carry

    def forward(i, carry):
        along(i).wait_recv()
        relay(i).start()
        return carry

    def finish(i, carry):
        along(i).wait_send()
        relay(i).wait()
        return carry

    lax.fori_loop(1, n // 2, start, 0)
    across(0, own_ref).start()
    keep.wait()
    lax.fori_loop(1, n // 2, forward, 0)
    across(0, own_ref).wait()
    lax.fori_loop(1, n // 2, finish, 0)


def gather_sp(block):
    n = lax.axis_size("sp")
    return pl.pallas_call(
        functools.partial(gather_kernel, n),
        out_shape=jax.ShapeDtypeStruct((n,) + block.shape, block.dtype),
        in_specs=[pl.BlockSpec(memory_space=pltpu.VMEM)],
        out_specs=pl.BlockSpec(memory_space=pltpu.VMEM),
        scratch_shapes=[
            pltpu.SemaphoreType.DMA((n // 2,)),
            pltpu.SemaphoreType.DMA((n // 2,)),
            pltpu.SemaphoreType.DMA((n // 2,)),
            pltpu.SemaphoreType.DMA((n // 2,)),
            pltpu.SemaphoreType.DMA,
        ],
        compiler_params=pltpu.CompilerParams(collective_id=0, has_side_effects=True),
        cost_estimate=pl.CostEstimate(flops=0, bytes_accessed=1 << 24, transcendentals=0),
        name="gather_kv",
    )(block)


def wide(value):
    return value.astype(jnp.float32)


def layer_kernel(names, *refs):
    r = SimpleNamespace(**dict(zip(names, refs)))
    sp = lax.axis_index("sp")
    tp = lax.axis_index("tp")
    z, x = sp // PAIR, lax.rem(sp, PAIR)
    y, c = tp // PAIR, lax.rem(tp, PAIR)
    ox, oy, oc = 1 - x, 1 - y, 1 - c
    width = r.residual.shape[1]
    half = r.residual.shape[0] // 2
    top, bottom = pl.ds(0, half), pl.ds(half, half)
    upper = z // 2
    folded = z + upper * (RING - 1 - 2 * z)

    def plane(o):
        return o + upper * (RING - 1 - 2 * o)

    groups = (z, plane(folded + 1), plane(2 - 2 * folded), plane(RING - 1))
    to_c = (sp, y * PAIR + oc)
    to_y = (sp, oy * PAIR + c)
    to_x = (z * PAIR + ox, tp)
    to_z = [None] + [(g * PAIR + x, tp) for g in groups[1:]]
    peers = [to_c, to_y, to_x] + to_z[1:]
    mine, xb, yb, db = x * PAIR + y, ox * PAIR + y, x * PAIR + oy, ox * PAIR + oy

    loads = [
        pltpu.make_async_copy(a, b, r.w_sem.at[i])
        for i, (a, b) in enumerate(
            ((r.wo_hbm, r.wo), (r.wg_hbm, r.wg), (r.wu_hbm, r.wu), (r.wd_hbm, r.wd))
        )
    ]
    for load in loads:
        load.start()
    barrier = pltpu.get_barrier_semaphore()
    for peer in peers:
        pl.semaphore_signal(barrier, inc=1, device_id=peer, device_id_type=MESH)

    started, inner_started = [], []
    inner = lax.rem(z + 1, RING) > 1
    outer = lax.rem(z + 1, RING) <= 1

    def remote(src, dst, s, t, to):
        return pltpu.make_async_remote_copy(
            src_ref=src, dst_ref=dst, send_sem=s, recv_sem=t, device_id=to, device_id_type=MESH
        )

    def send(src, dst, s, t, to):
        copy = remote(src, dst, s, t, to)
        copy.start()
        started.append(copy)
        return copy

    def passing(ref, s, t, p):
        return remote(ref, ref, s, t, to_z[1] if p == 2 else to_z[2])

    def narrow(value):
        return value.astype(jnp.bfloat16)

    tokens, heads, size = r.queries.shape
    kv_heads = r.keys.shape[1]
    kv_cols = kv_heads * size
    lane = lax.broadcasted_iota(jnp.int32, (tokens, size), 1)
    place = sp * tokens + lax.broadcasted_iota(jnp.int32, (tokens, size), 0)
    shift = GRID_W.bit_length() - 1
    quarter = size // 4
    index = jnp.where(lane < size // 2, lax.shift_right_logical(place, shift), place & (GRID_W - 1))
    freq = wide(lane & (quarter - 1))
    angle = wide(index) * jnp.exp(freq * (-math.log(rope_theta) / quarter))
    lower = (lane & quarter) == 0
    cosine = jnp.cos(angle)
    sine = jnp.where(lower, -jnp.sin(angle), jnp.sin(angle))

    def turned(value, gain):
        value = scale_rows(wide(value), gain)
        ahead = pltpu.roll(value, size - quarter, axis=value.ndim - 1)
        behind = pltpu.roll(value, quarter, axis=value.ndim - 1)
        if value.ndim == 2:
            return value * cosine + jnp.where(lower, ahead, behind) * sine
        low = (lax.broadcasted_iota(jnp.int32, value.shape, 2) & quarter) == 0
        return value * cosine[:, None] + jnp.where(low, ahead, behind) * sine[:, None]

    with jax.named_scope("keys"):
        for g in range(kv_heads):
            cols = pl.ds(g * size, size)
            r.kv[0, z, x, :, cols] = narrow(turned(r.keys[:, g, :], r.k_gain[...]))
            r.kv[1, z, x, :, cols] = r.values[:, g, :]
    pl.semaphore_wait(barrier, len(peers))
    def kv_at(p, i):
        return r.kv.at[i, groups[p], x]

    def kv_x(p, i):
        return remote(kv_at(p, i), kv_at(p, i), r.kx_s.at[p, i], r.kx_r.at[p, i], to_x)

    def kv_z(p, i, to):
        return remote(
            kv_at(p, i), kv_at(p, i), r.kz_s.at[p, i], r.kz_r.at[groups[p], i], to
        )

    def kv_pass(p, i):
        return passing(kv_at(p, i), r.kf_s.at[p, i], r.kz_r.at[groups[p], i], p)

    def kv_across(p, i):
        kv_z(p, i, to_z[1]).wait_recv()
        pl.when(inner)(kv_pass(p, i).start)
        kv_x(p, i).start()

    for i in range(2):
        kv_z(0, i, to_z[1]).start()
        pl.when(inner)(kv_pass(0, i).start)
        kv_x(0, i).start()
        started.append(kv_z(0, i, to_z[1]))
        started.extend(kv_x(p, i) for p in range(4))
        inner_started.extend(kv_pass(p, i) for p in range(4))
    with jax.named_scope("queries"):
        query = turned(r.queries[...], r.q_gain[...]) * size ** (-0.5)
        group_size = heads // kv_heads
        owner = lax.broadcasted_iota(jnp.int32, query.shape, 1) // group_size
        for g in range(kv_heads):
            r.query[:, pl.ds(g * size, size)] = narrow(
                jnp.where(owner == g, query, 0.0).reshape(tokens * heads, size)
            )
    spot = lax.broadcasted_iota(jnp.int32, (RING * PAIR, LANES), 1)
    expert = lax.broadcasted_iota(jnp.int32, spot.shape, 0)
    named = lax.broadcasted_iota(jnp.int32, (RING * PAIR, r.routes.shape[1]), 0)
    coef = jnp.zeros(named.shape, jnp.float32)
    for k in range(r.routes.shape[0]):
        hit = r.routes[k:k + 1, :] == named
        coef = coef + jnp.where(hit, r.route_weights[k:k + 1, :], 0.0)
    high = narrow(coef)
    low = narrow(coef - wide(high))

    def columns(value, offset):
        pick = narrow(jnp.where(spot == expert + offset, 1.0, 0.0))
        return lax.dot_general(
            value, pick, (((0,), (0,)), ((), ())), preferred_element_type=jnp.float32
        )

    r.got[z, c, mine, :, width:] = narrow(columns(high, 0) + columns(low, LANES // 2))
    row_step = min(tokens * heads, 256)

    def attend(p):
        for i in range(2):
            kv_x(p, i).wait_recv()

        @pl.loop(0, tokens * heads // row_step)
        def _(i):
            rows = pl.ds(pl.multiple_of(i * row_step, row_step), row_step)
            key = r.kv[0, groups[p]].reshape(PAIR * tokens, kv_cols)
            value = r.kv[1, groups[p]].reshape(PAIR * tokens, kv_cols)
            scores = lax.dot_general(
                r.query[rows, :], key, (((1,), (1,)), ((), ())),
                preferred_element_type=jnp.float32,
            )
            top_now = jnp.max(scores, axis=1, keepdims=True)
            if p:
                before = r.top[rows, :]
                top_now = jnp.maximum(before[:, :1], top_now)
            unnormed = jnp.exp(scores - top_now)
            total = jnp.sum(unnormed, axis=1, keepdims=True)
            both = jnp.dot(narrow(unnormed), value, preferred_element_type=jnp.float32)
            head = lax.rem(lax.broadcasted_iota(jnp.int32, (row_step, size), 0), heads)
            mixed = both[:, :size]
            for g in range(1, kv_heads):
                mixed = jnp.where(
                    head // group_size == g, both[:, g * size:(g + 1) * size], mixed
                )
            if p:
                rescale = jnp.exp(before - top_now)
                total = r.total[rows, :] * rescale + total
                mixed = r.mixed[rows, :] * rescale + mixed
            if p < 3:
                r.top[rows, :] = jnp.broadcast_to(top_now, (row_step, size))
                r.total[rows, :] = jnp.broadcast_to(total, (row_step, size))
                r.mixed[rows, :] = mixed
            else:
                r.mixed[rows, :] = mixed / total

    with jax.named_scope("attend"):
        for i in range(2):
            kv_across(1, i)
            pl.when(inner)(functools.partial(kv_across, 2, i))
        attend(0)
        for i in range(2):
            pl.when(outer)(functools.partial(kv_across, 2, i))
            pl.when(inner)(functools.partial(kv_across, 3, i))
        attend(1)
        for i in range(2):
            pl.when(outer)(functools.partial(kv_across, 3, i))
        attend(2)
        attend(3)
        for h in range(heads):
            r.heads[:, pl.ds(h * size, size)] = narrow(
                r.mixed[pl.ds(h, tokens, stride=heads), :]
            )
    loads[0].wait()
    tok = r.residual.shape[0]
    pieces = r.pc_s.shape[0]
    piece = width // pieces
    pair_copy, y_part = [], []
    def fold_pair(i):
        cols = pl.ds(i * piece, piece)
        pair_copy[i].wait_recv()
        r.py_out[:, cols] = narrow(wide(r.part[oy, c, :, cols]) + wide(r.pc_in[oy, :, cols]))
        y_part.append(
            send(r.py_out.at[:, cols], r.py_in.at[:, cols], r.py_s.at[i], r.py_r.at[i], to_y)
        )

    with jax.named_scope("proj"):
        for i in range(pieces):
            cols = pl.ds(i * piece, piece)
            part = jnp.dot(r.heads[...], r.wo[:, cols], preferred_element_type=jnp.float32)
            r.part[:, :, :, cols] = narrow(part).reshape(PAIR, PAIR, tok, piece)
            pair_copy.append(
                send(
                    r.part.at[:, oc, :, cols], r.pc_in.at[:, :, cols],
                    r.pc_s.at[i], r.pc_r.at[i], to_c,
                )
            )
            if i:
                fold_pair(i - 1)
        fold_pair(pieces - 1)
        for i in range(pieces):
            y_part[i].wait_recv()
        projected = wide(r.part[y, c]) + wide(r.pc_in[y]) + wide(r.py_in[...])
        mid = wide(r.residual[...]) + scale_rows(projected, r.gain_mix[...])
        r.middle[...] = mid
        r.got[z, c, mine, :, 0:width] = narrow(scale_rows(mid, r.gain_pre[...]))

    def block(p, k, rows=slice(None)):
        return r.got.at[groups[p], c, k, rows]

    hx_copy, hy_copy = [None] * 4, [None] * 4

    def relay(p, k, slot):
        return remote(block(p, k), block(p, k), r.c_s.at[p, slot], r.c_r.at[p, slot], to_c)

    def along_x(p):
        return remote(block(p, mine), block(p, mine), r.x_s.at[p], r.x_r.at[p], to_x)

    def along_y(p):
        return remote(block(p, mine), block(p, mine), r.y_s.at[p], r.y_r.at[p], to_y)

    def along_z(p):
        return remote(
            block(p, mine), block(p, mine), r.z_s.at[p], r.z_r.at[groups[p]], to_z[1]
        )

    def block_pass(p):
        return passing(block(p, mine), r.zf_s.at[p], r.z_r.at[groups[p]], p)

    def spread(p):
        if p:
            along_z(p).wait_recv()
        else:
            along_z(p).start()
        pl.when(inner)(block_pass(p).start)
        along_x(p).start()
        along_y(p).start()
        relay(p, mine, 0).start()

    started.append(along_z(0))
    for p in range(4):
        inner_started.append(block_pass(p))
        started += [along_x(p), along_y(p)]
        started += [relay(p, k, i) for i, k in enumerate((mine, xb, yb, db))]

    def cross(p):
        along_x(p).wait_recv()
        hy_copy[p] = send(
            block(p, xb, top), block(p, xb, top), r.hy_s.at[p], r.hy_r.at[p], to_y
        )
        relay(p, xb, 1).start()
        along_y(p).wait_recv()
        hx_copy[p] = send(
            block(p, yb, bottom), block(p, yb, bottom), r.hx_s.at[p], r.hx_r.at[p], to_x
        )
        relay(p, yb, 2).start()

    def corner(p):
        hx_copy[p].wait_recv()
        hy_copy[p].wait_recv()
        relay(p, db, 3).start()

    per = r.got.shape[2] * r.got.shape[3]

    def serve(p):
        for i, k in enumerate((mine, xb, yb, db)):
            relay(p, k, i).wait_recv()
        g = groups[p]
        spread_w = wide(r.got[g, :, :, :, width:].reshape(2 * per, LANES))
        lane = lax.broadcasted_iota(jnp.int32, spread_w.shape, 1)
        chosen = lax.rem(lane, LANES // 2) == sp
        coef = jnp.sum(jnp.where(chosen, spread_w, 0.0), axis=1, keepdims=True)
        step = min(r.wg.shape[1], 256)

        @pl.loop(0, r.wg.shape[1] // step)
        def _(i):
            cols = pl.ds(pl.multiple_of(i * step, step), step)
            rows = r.got[g, :, :, :, 0:width].reshape(2 * per, width)
            gate = jnp.dot(rows, r.wg[:, cols], preferred_element_type=jnp.float32)
            up = jnp.dot(rows, r.wu[:, cols], preferred_element_type=jnp.float32)
            gate = jnp.minimum(gate, clamp_limit)
            up = jnp.clip(up, -clamp_limit, clamp_limit)
            r.active[:, cols] = narrow(gate * jax.nn.sigmoid(swish_alpha * gate) * (up + 1.0))

        @pl.loop(0, width // 512)
        def _(i):
            cols = pl.ds(pl.multiple_of(i * 512, 512), 512)
            down = jnp.dot(r.active[...], r.wd[:, cols], preferred_element_type=jnp.float32)
            r.partial[p, :, :, :, cols] = narrow(down * coef).reshape(
                r.partial.shape[1:4] + (512,)
            )

        back[p] = send(r.partial.at[p, oc], r.core_in.at[p], r.rc_s.at[p], r.rc_r.at[p], to_c)

    back = [None] * 4
    dx_copy, dy_copy = [None] * 4, [None] * 4
    bx_copy, by_copy = [[] for _ in range(4)], [[] for _ in range(4)]
    home = [None] * 4

    def give_x(p, i, rows):
        bx_copy[p].append(
            send(
                r.summed.at[p, xb, rows], r.x_in.at[p, rows],
                r.bx_s.at[p, i], r.bx_r.at[p, i], to_x,
            )
        )

    def give_y(p, i, rows):
        by_copy[p].append(
            send(
                r.summed.at[p, yb, rows], r.y_in.at[p, rows],
                r.by_s.at[p, i], r.by_r.at[p, i], to_y,
            )
        )

    def fold(p):
        back[p].wait_recv()
        for k in (db, xb, yb, mine):
            r.summed[p, k] = narrow(wide(r.partial[p, c, k]) + wide(r.core_in[p, k]))
        dx_copy[p] = send(
            r.summed.at[p, db, top], r.dx_in.at[p], r.dx_s.at[p], r.dx_r.at[p], to_x
        )
        dy_copy[p] = send(
            r.summed.at[p, db, bottom], r.dy_in.at[p], r.dy_s.at[p], r.dy_r.at[p], to_y
        )
        give_x(p, 0, top)
        give_y(p, 0, bottom)

    def join(p):
        dx_copy[p].wait_recv()
        r.summed[p, yb, top] = narrow(wide(r.summed[p, yb, top]) + wide(r.dx_in[p]))
        give_y(p, 1, top)
        dy_copy[p].wait_recv()
        r.summed[p, xb, bottom] = narrow(wide(r.summed[p, xb, bottom]) + wide(r.dy_in[p]))
        give_x(p, 1, bottom)

    def gather(p):
        for copy in bx_copy[p] + by_copy[p]:
            copy.wait_recv()
        return wide(r.summed[p, mine]) + wide(r.x_in[p]) + wide(r.y_in[p])

    def leave(p):
        r.home_out[p] = narrow(gather(p))
        home[p] = send(
            r.home_out.at[p], r.home_in.at[z], r.b_s.at[p], r.b_r.at[z], to_z[p]
        )

    with jax.named_scope("spread"):
        spread(0)
        cross(0)
        spread(1)
        pl.when(inner)(functools.partial(spread, 2))
        corner(0)
        pl.when(outer)(functools.partial(spread, 2))
        pl.when(inner)(functools.partial(spread, 3))
    for load in loads[1:]:
        load.wait()
    with jax.named_scope("serve"):
        serve(0)
        cross(1)
        pl.when(outer)(functools.partial(spread, 3))
        corner(1)
        cross(2)
        fold(0)
        serve(1)
        join(0)
        corner(2)
        cross(3)
        fold(1)
        serve(2)
        join(1)
        corner(3)
        fold(2)
        serve(3)
        leave(1)
        join(2)
        fold(3)
        leave(2)
        join(3)
        mixture = gather(0)
        leave(3)
    with jax.named_scope("back"):
        for p in range(1, 4):
            g = groups[p]
            pltpu.make_async_remote_copy(
                src_ref=r.home_out.at[p], dst_ref=r.home_in.at[g], send_sem=r.b_s.at[p],
                recv_sem=r.b_r.at[g], device_id=to_z[p], device_id_type=MESH,
            ).wait_recv()
            mixture = mixture + wide(r.home_in[g])
        r.out[...] = (r.middle[...] + scale_rows(mixture, r.gain_moe[...])).astype(r.out.dtype)
        for copy in started:
            copy.wait_send()

        @pl.when(inner)
        def _():
            for copy in inner_started:
                copy.wait_send()


def whole_layer(
    queries, keys, values, q_gain, k_gain, w_out, residual, gain_mix, gain_pre, routes,
    route_weights, w_gate, w_up, w_down, gain_moe,
):
    tokens, heads, size = queries.shape
    kv_cols = keys.shape[1] * size
    tok, width = residual.shape
    ff = w_gate.shape[1]
    full = width + LANES
    blocks = PAIR * PAIR
    half = tok // 2
    pieces = 2
    bf, f32 = jnp.bfloat16, jnp.float32
    dma = pltpu.SemaphoreType.DMA
    here = pl.BlockSpec(memory_space=pltpu.VMEM)
    there = pl.BlockSpec(memory_space=pl.ANY)
    scratch = {
        "kv": pltpu.VMEM((2, RING, PAIR, tokens, kv_cols), bf),
        "query": pltpu.VMEM((tokens * heads, kv_cols), bf),
        "top": pltpu.VMEM((tokens * heads, size), f32),
        "total": pltpu.VMEM((tokens * heads, size), f32),
        "mixed": pltpu.VMEM((tokens * heads, size), f32),
        "heads": pltpu.VMEM((tokens, heads * size), bf),
        "wo": pltpu.VMEM((heads * size, width), bf),
        "part": pltpu.VMEM((PAIR, PAIR, tok, width), bf),
        "wg": pltpu.VMEM((width, ff), bf),
        "wu": pltpu.VMEM((width, ff), bf),
        "wd": pltpu.VMEM((ff, width), bf),
        "pc_in": pltpu.VMEM((PAIR, tok, width), bf),
        "py_out": pltpu.VMEM((tok, width), bf),
        "py_in": pltpu.VMEM((tok, width), bf),
        "got": pltpu.VMEM((RING, PAIR, blocks, tok, full), bf),
        "middle": pltpu.VMEM((tok, width), f32),
        "active": pltpu.VMEM((PAIR * blocks * tok, ff), bf),
        "partial": pltpu.VMEM((RING, PAIR, blocks, tok, width), bf),
        "core_in": pltpu.VMEM((RING, blocks, tok, width), bf),
        "summed": pltpu.VMEM((RING, blocks, tok, width), bf),
        "dx_in": pltpu.VMEM((RING, half, width), bf),
        "dy_in": pltpu.VMEM((RING, half, width), bf),
        "x_in": pltpu.VMEM((RING, tok, width), bf),
        "y_in": pltpu.VMEM((RING, tok, width), bf),
        "home_out": pltpu.VMEM((RING, tok, width), bf),
        "home_in": pltpu.VMEM((RING, tok, width), bf),
        "w_sem": dma((4,)),
    }
    for name, dims in (
        ("kz", (4, 2)), ("kx", (4, 2)), ("kf", (4, 2)), ("zf", (4,)), ("pc", (pieces,)), ("py", (pieces,)), ("z", (4,)), ("x", (4,)), ("y", (4,)), ("hx", (4,)),
        ("hy", (4,)), ("c", (4, 4)), ("rc", (4,)), ("dx", (4,)), ("dy", (4,)), ("bx", (4, 2)),
        ("by", (4, 2)), ("b", (4,)),
    ):
        scratch[name + "_s"] = dma(dims)
        scratch[name + "_r"] = dma(dims)
    operands = (
        "queries", "keys", "values", "q_gain", "k_gain", "residual", "gain_mix", "gain_pre",
        "gain_moe", "routes", "route_weights", "wo_hbm", "wg_hbm", "wu_hbm", "wd_hbm",
    )
    names = operands + ("out",) + tuple(scratch)
    return pl.pallas_call(
        functools.partial(layer_kernel, names),
        out_shape=jax.ShapeDtypeStruct((tok, width), bf),
        in_specs=[here] * 11 + [there] * 4,
        out_specs=here,
        scratch_shapes=list(scratch.values()),
        compiler_params=pltpu.CompilerParams(
            collective_id=1, has_side_effects=True, vmem_limit_bytes=56 << 20
        ),
        name="whole_layer",
    )(
        queries, keys, values, q_gain, k_gain, residual, gain_mix, gain_pre, gain_moe, routes,
        route_weights, w_out, w_gate, w_up, w_down,
    )


def on_device(
    queries,
    keys,
    values,
    q_gain,
    k_gain,
    w_out,
    residual,
    gain_mix,
    gain_pre,
    routes,
    route_weights,
    w_gate,
    w_up,
    w_down,
    gain_moe,
):
    local_experts = w_gate.shape[0]
    experts_all = local_experts * lax.axis_size("sp")
    tok_part, width = residual.shape
    capacity = max(2, (2 * tok_part * TOP + experts_all - 1) // experts_all)
    grid_fits = lax.axis_size("sp") == RING * PAIR and lax.axis_size("tp") == PAIR * PAIR
    if grid_fits and local_experts == 1 and capacity >= tok_part:
        return whole_layer(
            queries, keys, values, q_gain[None], k_gain[None], w_out, residual,
            gain_mix[None], gain_pre[None], routes.T, route_weights.T, w_gate[0], w_up[0],
            w_down[0], gain_moe[None],
        )
    tok_rows, head_local, head_size = queries.shape
    kv_local = keys.shape[1]
    group_size = head_local // kv_local
    positions = lax.axis_index("sp") * tok_rows + jnp.arange(tok_rows, dtype=jnp.int32)
    cosine_table, sine_table = rope_tables(positions, head_size)
    q_turned = (
        turn(scale_rows(queries.astype(jnp.float32), q_gain), cosine_table, sine_table)
        * head_size ** (-0.5)
    ).astype(jnp.bfloat16)
    k_turned = turn(scale_rows(keys.astype(jnp.float32), k_gain), cosine_table, sine_table).astype(
        jnp.bfloat16
    )
    q_grouped = q_turned.reshape(tok_rows, kv_local, group_size, head_size)
    initial = (
        jnp.full((kv_local, group_size, tok_rows), -jnp.inf, jnp.float32),
        jnp.zeros((kv_local, group_size, tok_rows), jnp.float32),
        jnp.zeros((kv_local, group_size, tok_rows, head_size), jnp.float32),
    )
    carry_state = initial
    kv_cols = kv_local * head_size
    both = gather_sp(
        jnp.concatenate(
            [k_turned.reshape(tok_rows, kv_cols), values.reshape(tok_rows, kv_cols)], axis=1
        )
    ).reshape(-1, 2 * kv_cols)
    key_piece = both[:, :kv_cols].reshape(-1, kv_local, head_size)
    value_piece = both[:, kv_cols:].reshape(-1, kv_local, head_size)
    piece_rows = key_piece.shape[0]
    block_rows = math.gcd(piece_rows, 1024)
    key_blocks = key_piece.reshape(piece_rows // block_rows, block_rows, kv_local, head_size)
    value_blocks = value_piece.reshape(piece_rows // block_rows, block_rows, kv_local, head_size)

    def absorb_block(state_now, key_value):
        running_max, running_sum, weighted = state_now
        key_block, value_block = key_value
        scores = jnp.einsum(
            "qkgd,skd->kgqs", q_grouped, key_block, preferred_element_type=jnp.float32
        )
        new_max = jnp.maximum(running_max, jnp.max(scores, axis=-1))
        rescale = jnp.exp(running_max - new_max)
        unnorm = jnp.exp(scores - new_max[..., None])
        running_sum = running_sum * rescale + jnp.sum(unnorm, axis=-1)
        weighted = weighted * rescale[..., None] + jnp.einsum(
            "kgqs,skd->kgqd",
            unnorm.astype(jnp.bfloat16),
            value_block,
            preferred_element_type=jnp.float32,
        )
        return ((new_max, running_sum, weighted), None)

    carry_state, ignored = lax.scan(absorb_block, carry_state, (key_blocks, value_blocks))
    running_max, running_sum, weighted = carry_state
    mixed_heads = (weighted / running_sum[..., None]).transpose(2, 0, 1, 3)
    mixed_heads = mixed_heads.reshape(tok_rows, head_local * head_size).astype(jnp.bfloat16)
    part = jnp.dot(mixed_heads, w_out, preferred_element_type=jnp.float32).astype(jnp.bfloat16)
    projected = lax.psum_scatter(
        part,
        "tp",
        scatter_dimension=0,
        tiled=True,
    ).astype(jnp.float32)
    middle = residual.astype(jnp.float32) + scale_rows(projected, gain_mix)
    normed = scale_rows(middle, gain_pre).astype(jnp.bfloat16)
    tables = slot_table(routes, experts_all, capacity)
    chosen = jnp.sum(tables, axis=1)
    outbound = jnp.einsum("tp,td->pd", chosen, normed, preferred_element_type=jnp.float32)
    outbound = outbound.astype(jnp.bfloat16).reshape(experts_all, capacity, width)
    arrived_rows = lax.all_gather(
        lax.all_to_all(outbound, "sp", split_axis=0, concat_axis=0, tiled=True),
        "tp",
        axis=0,
        tiled=True,
    )
    leading = arrived_rows.shape[0] // local_experts
    partial_value = expert_apply(
        arrived_rows.reshape(leading, local_experts, arrived_rows.shape[1], width),
        w_gate,
        w_up,
        w_down,
    )
    summed = lax.psum_scatter(
        partial_value.reshape(arrived_rows.shape).astype(jnp.bfloat16),
        "tp",
        scatter_dimension=0,
        tiled=True,
    )
    returned = send_back(summed)
    gathered = jnp.einsum(
        "tkp,pd->tkd",
        tables,
        returned.reshape(experts_all * capacity, width),
        preferred_element_type=jnp.float32,
    )
    mixture = jnp.sum(gathered * route_weights[:, :, None], axis=1)
    return (middle + scale_rows(mixture, gain_moe)).astype(jnp.bfloat16)


def solution(mesh):
    placed = (
        P("sp", "tp", None),
        P("sp", "tp", None),
        P("sp", "tp", None),
        P(),
        P(),
        P("tp", None),
        P(("sp", "tp"), None),
        P(),
        P(),
        P(("sp", "tp"), None),
        P(("sp", "tp"), None),
        P("sp", None, "tp"),
        P("sp", None, "tp"),
        P("sp", "tp", None),
        P(),
    )
    return jax.shard_map(
        on_device, mesh=mesh, in_specs=placed, out_specs=P(("sp", "tp"), None), check_vma=False
    )
```

```python
import functools
import math
from types import SimpleNamespace

import jax
import jax.numpy as jnp
from jax import lax
from jax.experimental import pallas as pl
from jax.experimental.pallas import tpu as pltpu
from jax.sharding import PartitionSpec as P

TOP = 4
GRID_W = 64


norm_eps = 1e-06
rope_theta = 10000.0
clamp_limit = 7.0
swish_alpha = 1.702


def rope_tables(positions, head_size):
    row_index = (positions // GRID_W).astype(jnp.float32)
    col_index = (positions % GRID_W).astype(jnp.float32)
    freq_count = head_size // 4
    inverse = rope_theta ** (-jnp.arange(freq_count, dtype=jnp.float32) / freq_count)
    angles = jnp.stack([row_index[:, None] * inverse, col_index[:, None] * inverse], axis=1)
    return (jnp.cos(angles), jnp.sin(angles))


def turn(array_in, cosine_table, sine_table):
    token_count, head_count, head_size = array_in.shape
    split_field = array_in.reshape(token_count, head_count, 2, 2, head_size // 4)
    first_half = split_field[:, :, :, 0, :]
    second_half = split_field[:, :, :, 1, :]
    cos_wide = cosine_table[:, None]
    sin_wide = sine_table[:, None]
    turned = jnp.stack(
        [
            first_half * cos_wide - second_half * sin_wide,
            second_half * cos_wide + first_half * sin_wide,
        ],
        axis=3,
    )
    return turned.reshape(token_count, head_count, head_size)


def scale_rows(array_in, gain_vec):
    return (
        array_in
        * lax.rsqrt(jnp.mean(array_in * array_in, axis=-1, keepdims=True) + norm_eps)
        * gain_vec
    )


def slot_table(route_rows, experts, capacity):
    flat_routes = route_rows.reshape(-1)
    expert_hits = (flat_routes[:, None] == jnp.arange(experts, dtype=jnp.int32)[None, :]).astype(
        jnp.int32
    )
    slot_index = jnp.sum((jnp.cumsum(expert_hits, axis=0) - expert_hits) * expert_hits, axis=1)
    target = flat_routes * capacity + slot_index
    slot_onehot = target[:, None] == jnp.arange(experts * capacity, dtype=jnp.int32)[None, :]
    return slot_onehot.astype(jnp.bfloat16).reshape(
        route_rows.shape[0], route_rows.shape[1], experts * capacity
    )


def expert_apply(arrived_rows, w_gate, w_up, w_down):
    gate_pre = jnp.minimum(
        jnp.einsum("serd,edf->serf", arrived_rows, w_gate, preferred_element_type=jnp.float32),
        clamp_limit,
    )
    up_pre = jnp.clip(
        jnp.einsum("serd,edf->serf", arrived_rows, w_up, preferred_element_type=jnp.float32),
        -clamp_limit,
        clamp_limit,
    )
    active = (gate_pre * jax.nn.sigmoid(swish_alpha * gate_pre) * (up_pre + 1.0)).astype(
        jnp.bfloat16
    )
    partial_value = jnp.einsum("serf,efd->serd", active, w_down, preferred_element_type=jnp.float32)
    return lax.optimization_barrier(partial_value.astype(jnp.bfloat16)).astype(jnp.float32)


def send_back(finished):
    return lax.all_to_all(finished, "sp", split_axis=0, concat_axis=0, tiled=True)


MESH = pl.DeviceIdType.MESH
RING = 4
PAIR = 2
LANES = 128


def gather_kernel(n, own_ref, out_ref, send_sem, recv_sem, pass_sem, take_sem, own_sem):
    me = lax.axis_index("sp")
    tp = lax.axis_index("tp")
    pair = me + 1 - 2 * lax.rem(me, 2)
    barrier = pltpu.get_barrier_semaphore()

    def greet(i, carry):
        pl.semaphore_signal(
            barrier, inc=1, device_id=(lax.rem(me + 2 * i, n), tp), device_id_type=MESH
        )
        return carry

    lax.fori_loop(1, n // 2, greet, 0)
    pl.semaphore_signal(barrier, inc=1, device_id=(pair, tp), device_id_type=MESH)
    keep = pltpu.make_async_copy(own_ref, out_ref.at[me], own_sem)
    keep.start()
    pl.semaphore_wait(barrier, n // 2)

    def along(i):
        return pltpu.make_async_remote_copy(
            src_ref=own_ref,
            dst_ref=out_ref.at[me],
            send_sem=send_sem.at[i],
            recv_sem=recv_sem.at[i],
            device_id=(lax.rem(me + 2 * i, n), tp),
            device_id_type=MESH,
        )

    def across(i, src):
        return pltpu.make_async_remote_copy(
            src_ref=src,
            dst_ref=out_ref.at[lax.rem(me + n - 2 * i, n)],
            send_sem=pass_sem.at[i],
            recv_sem=take_sem.at[i],
            device_id=(pair, tp),
            device_id_type=MESH,
        )

    def relay(i):
        return across(i, out_ref.at[lax.rem(me + n - 2 * i, n)])

    def start(i, carry):
        along(i).start()
        return carry

    def forward(i, carry):
        along(i).wait_recv()
        relay(i).start()
        return carry

    def finish(i, carry):
        along(i).wait_send()
        relay(i).wait()
        return carry

    lax.fori_loop(1, n // 2, start, 0)
    across(0, own_ref).start()
    keep.wait()
    lax.fori_loop(1, n // 2, forward, 0)
    across(0, own_ref).wait()
    lax.fori_loop(1, n // 2, finish, 0)


def gather_sp(block):
    n = lax.axis_size("sp")
    return pl.pallas_call(
        functools.partial(gather_kernel, n),
        out_shape=jax.ShapeDtypeStruct((n,) + block.shape, block.dtype),
        in_specs=[pl.BlockSpec(memory_space=pltpu.VMEM)],
        out_specs=pl.BlockSpec(memory_space=pltpu.VMEM),
        scratch_shapes=[
            pltpu.SemaphoreType.DMA((n // 2,)),
            pltpu.SemaphoreType.DMA((n // 2,)),
            pltpu.SemaphoreType.DMA((n // 2,)),
            pltpu.SemaphoreType.DMA((n // 2,)),
            pltpu.SemaphoreType.DMA,
        ],
        compiler_params=pltpu.CompilerParams(collective_id=0, has_side_effects=True),
        cost_estimate=pl.CostEstimate(flops=0, bytes_accessed=1 << 24, transcendentals=0),
        name="gather_kv",
    )(block)


def wide(value):
    return value.astype(jnp.float32)


def layer_kernel(names, *refs):
    r = SimpleNamespace(**dict(zip(names, refs)))
    sp = lax.axis_index("sp")
    tp = lax.axis_index("tp")
    z, x = sp // PAIR, lax.rem(sp, PAIR)
    y, c = tp // PAIR, lax.rem(tp, PAIR)
    ox, oy, oc = 1 - x, 1 - y, 1 - c
    width = r.residual.shape[1]
    half = r.residual.shape[0] // 2
    top, bottom = pl.ds(0, half), pl.ds(half, half)
    upper = z // 2
    folded = z + upper * (RING - 1 - 2 * z)

    def plane(o):
        return o + upper * (RING - 1 - 2 * o)

    groups = (z, plane(folded + 1), plane(2 - 2 * folded), plane(RING - 1))
    to_c = (sp, y * PAIR + oc)
    to_y = (sp, oy * PAIR + c)
    to_x = (z * PAIR + ox, tp)
    to_z = [None] + [(g * PAIR + x, tp) for g in groups[1:]]
    peers = [to_c, to_y, to_x] + to_z[1:]
    mine, xb, yb, db = x * PAIR + y, ox * PAIR + y, x * PAIR + oy, ox * PAIR + oy

    loads = [
        pltpu.make_async_copy(a, b, r.w_sem.at[i])
        for i, (a, b) in enumerate(
            (
                (r.wo_hbm, r.wo),
                (r.wg_hbm, r.wg.at[0]),
                (r.wu_hbm, r.wu.at[0]),
                (r.wd_hbm, r.wd.at[0]),
            )
        )
    ]
    for load in loads:
        load.start()
    barrier = pltpu.get_barrier_semaphore()
    for peer in peers:
        pl.semaphore_signal(barrier, inc=1, device_id=peer, device_id_type=MESH)

    started, inner_started = [], []
    inner = lax.rem(z + 1, RING) > 1
    outer = lax.rem(z + 1, RING) <= 1

    def remote(src, dst, s, t, to):
        return pltpu.make_async_remote_copy(
            src_ref=src, dst_ref=dst, send_sem=s, recv_sem=t, device_id=to, device_id_type=MESH
        )

    def send(src, dst, s, t, to):
        copy = remote(src, dst, s, t, to)
        copy.start()
        started.append(copy)
        return copy

    def passing(ref, s, t, p):
        return remote(ref, ref, s, t, to_z[1] if p == 2 else to_z[2])

    def narrow(value):
        return value.astype(jnp.bfloat16)

    tokens, heads, size = r.queries.shape
    kv_heads = r.keys.shape[1]
    kv_cols = kv_heads * size
    lane = lax.broadcasted_iota(jnp.int32, (tokens, size), 1)
    place = sp * tokens + lax.broadcasted_iota(jnp.int32, (tokens, size), 0)
    shift = GRID_W.bit_length() - 1
    quarter = size // 4
    index = jnp.where(lane < size // 2, lax.shift_right_logical(place, shift), place & (GRID_W - 1))
    freq = wide(lane & (quarter - 1))
    angle = wide(index) * jnp.exp(freq * (-math.log(rope_theta) / quarter))
    lower = (lane & quarter) == 0
    cosine = jnp.cos(angle)
    sine = jnp.where(lower, -jnp.sin(angle), jnp.sin(angle))

    def turned(value, gain):
        value = scale_rows(wide(value), gain)
        ahead = pltpu.roll(value, size - quarter, axis=value.ndim - 1)
        behind = pltpu.roll(value, quarter, axis=value.ndim - 1)
        if value.ndim == 2:
            return value * cosine + jnp.where(lower, ahead, behind) * sine
        low = (lax.broadcasted_iota(jnp.int32, value.shape, 2) & quarter) == 0
        return value * cosine[:, None] + jnp.where(low, ahead, behind) * sine[:, None]

    with jax.named_scope("keys"):
        for g in range(kv_heads):
            cols = pl.ds(g * size, size)
            r.kv[0, z, x, :, cols] = narrow(turned(r.keys[:, g, :], r.k_gain[...]))
            r.kv[1, z, x, :, cols] = r.values[:, g, :]
    pl.semaphore_wait(barrier, len(peers))
    def kv_at(p, i):
        return r.kv.at[i, groups[p], x]

    def kv_x(p, i):
        return remote(kv_at(p, i), kv_at(p, i), r.kx_s.at[p, i], r.kx_r.at[p, i], to_x)

    def kv_z(p, i, to):
        return remote(
            kv_at(p, i), kv_at(p, i), r.kz_s.at[p, i], r.kz_r.at[groups[p], i], to
        )

    def kv_pass(p, i):
        return passing(kv_at(p, i), r.kf_s.at[p, i], r.kz_r.at[groups[p], i], p)

    def kv_across(p, i):
        kv_z(p, i, to_z[1]).wait_recv()
        pl.when(inner)(kv_pass(p, i).start)
        kv_x(p, i).start()

    for i in range(2):
        kv_z(0, i, to_z[1]).start()
        pl.when(inner)(kv_pass(0, i).start)
        kv_x(0, i).start()
        started.append(kv_z(0, i, to_z[1]))
        started.extend(kv_x(p, i) for p in range(4))
        inner_started.extend(kv_pass(p, i) for p in range(4))
    with jax.named_scope("queries"):
        query = turned(r.queries[...], r.q_gain[...]) * size ** (-0.5)
        group_size = heads // kv_heads
        owner = lax.broadcasted_iota(jnp.int32, query.shape, 1) // group_size
        for g in range(kv_heads):
            r.query[:, pl.ds(g * size, size)] = narrow(
                jnp.where(owner == g, query, 0.0).reshape(tokens * heads, size)
            )
    spot = lax.broadcasted_iota(jnp.int32, (RING * PAIR, LANES), 1)
    expert = lax.broadcasted_iota(jnp.int32, spot.shape, 0)
    named = lax.broadcasted_iota(jnp.int32, (RING * PAIR, r.routes.shape[1]), 0)
    coef = jnp.zeros(named.shape, jnp.float32)
    for k in range(r.routes.shape[0]):
        hit = r.routes[k:k + 1, :] == named
        coef = coef + jnp.where(hit, r.route_weights[k:k + 1, :], 0.0)
    high = narrow(coef)
    low = narrow(coef - wide(high))

    def columns(value, offset):
        pick = narrow(jnp.where(spot == expert + offset, 1.0, 0.0))
        return lax.dot_general(
            value, pick, (((0,), (0,)), ((), ())), preferred_element_type=jnp.float32
        )

    r.got[z, mine, :, width:] = narrow(columns(high, 0) + columns(low, LANES // 2))
    row_step = min(tokens * heads, 256)

    def attend(p, part):
        if part != 1:
            for i in range(2):
                kv_x(p, i).wait_recv()
        steps = tokens * heads // row_step
        span = {0: (0, steps // 2), 1: (steps // 2, steps), 2: (0, steps)}[part]

        @pl.loop(*span)
        def _(i):
            rows = pl.ds(pl.multiple_of(i * row_step, row_step), row_step)
            key = r.kv[0, groups[p]].reshape(PAIR * tokens, kv_cols)
            value = r.kv[1, groups[p]].reshape(PAIR * tokens, kv_cols)
            scores = lax.dot_general(
                r.query[rows, :], key, (((1,), (1,)), ((), ())),
                preferred_element_type=jnp.float32,
            )
            top_now = jnp.max(scores, axis=1, keepdims=True)
            if p:
                before = r.top[rows, :]
                top_now = jnp.maximum(before[:, :1], top_now)
            unnormed = jnp.exp(scores - top_now)
            total = jnp.sum(unnormed, axis=1, keepdims=True)
            both = jnp.dot(narrow(unnormed), value, preferred_element_type=jnp.float32)
            head = lax.rem(lax.broadcasted_iota(jnp.int32, (row_step, size), 0), heads)
            mixed = both[:, :size]
            for g in range(1, kv_heads):
                mixed = jnp.where(
                    head // group_size == g, both[:, g * size:(g + 1) * size], mixed
                )
            if p:
                rescale = jnp.exp(before - top_now)
                total = r.total[rows, :] * rescale + total
                mixed = r.mixed[rows, :] * rescale + mixed
            if p < 3:
                r.top[rows, :] = jnp.broadcast_to(top_now, (row_step, size))
                r.total[rows, :] = jnp.broadcast_to(total, (row_step, size))
                r.mixed[rows, :] = mixed
            else:
                r.mixed[rows, :] = mixed / total

    shared = []

    def share():
        for i, ref in enumerate((r.wg, r.wu, r.wd)):
            loads[i + 1].wait()
            shared.append(send(ref.at[0], ref.at[1], r.w_s.at[i], r.w_r.at[i], to_c))

    with jax.named_scope("attend"):
        for i in range(2):
            kv_across(1, i)
            pl.when(inner)(functools.partial(kv_across, 2, i))
        attend(0, 0)
        pl.when(outer)(functools.partial(kv_across, 2, 0))
        pl.when(inner)(functools.partial(kv_across, 3, 0))
        attend(0, 1)
        pl.when(outer)(functools.partial(kv_across, 2, 1))
        pl.when(inner)(functools.partial(kv_across, 3, 1))
        pl.when(outer)(functools.partial(kv_across, 3, 0))
        share()
        attend(1, 0)
        pl.when(outer)(functools.partial(kv_across, 3, 1))
        attend(1, 1)
        attend(2, 2)
        attend(3, 2)
        for h in range(heads):
            r.heads[:, pl.ds(h * size, size)] = narrow(
                r.mixed[pl.ds(h, tokens, stride=heads), :]
            )
    loads[0].wait()
    tok = r.residual.shape[0]
    pieces = r.pc_s.shape[0]
    piece = width // pieces
    pair_copy, y_part = [], []
    def fold_pair(i):
        cols = pl.ds(i * piece, piece)
        pair_copy[i].wait_recv()
        r.py_out[:, cols] = narrow(wide(r.part[oy, c, :, cols]) + wide(r.pc_in[oy, :, cols]))
        y_part.append(
            send(r.py_out.at[:, cols], r.py_in.at[:, cols], r.py_s.at[i], r.py_r.at[i], to_y)
        )

    with jax.named_scope("proj"):
        for i in range(pieces):
            cols = pl.ds(i * piece, piece)
            part = jnp.dot(r.heads[...], r.wo[:, cols], preferred_element_type=jnp.float32)
            r.part[:, :, :, cols] = narrow(part).reshape(PAIR, PAIR, tok, piece)
            pair_copy.append(
                send(
                    r.part.at[:, oc, :, cols], r.pc_in.at[:, :, cols],
                    r.pc_s.at[i], r.pc_r.at[i], to_c,
                )
            )
            if i:
                fold_pair(i - 1)
        fold_pair(pieces - 1)
        for i in range(pieces):
            y_part[i].wait_recv()
        projected = wide(r.part[y, c]) + wide(r.pc_in[y]) + wide(r.py_in[...])
        mid = wide(r.residual[...]) + scale_rows(projected, r.gain_mix[...])
        r.middle[...] = mid
        r.got[z, mine, :, 0:width] = narrow(scale_rows(mid, r.gain_pre[...]))

    def block(p, k, rows=slice(None)):
        return r.got.at[groups[p], k, rows]

    through = (0, RING - 1)

    ends = (top, bottom)

    def along_x(p, i):
        ref = block(p, mine, ends[i])
        return remote(ref, ref, r.x_s.at[p, i], r.x_r.at[p, i], to_x)

    def along_y(p, i):
        ref = block(p, mine, ends[i])
        return remote(ref, ref, r.y_s.at[p, i], r.y_r.at[p, i], to_y)

    def along_z(p, i):
        ref = block(p, mine, ends[i])
        return remote(ref, ref, r.z_s.at[p, i], r.z_r.at[groups[p], i], to_z[1])

    def block_pass(p, i):
        return passing(block(p, mine, ends[i]), r.zf_s.at[p, i], r.z_r.at[groups[p], i], p)

    def corner_z(p):
        return remote(block(p, db), block(p, db), r.d_s.at[p], r.d_r.at[groups[p]], to_z[1])

    def corner_pass(p):
        return passing(block(p, db), r.df_s.at[p], r.d_r.at[groups[p]], p)

    def half_x(p):
        ref = block(p, yb, bottom)
        return remote(ref, ref, r.hx_s.at[p], r.hx_r.at[p], to_x)

    def half_y(p):
        ref = block(p, xb, top)
        return remote(ref, ref, r.hy_s.at[p], r.hy_r.at[p], to_y)

    def begin():
        for i in range(2):
            along_z(0, i).start()
            pl.when(inner)(block_pass(0, i).start)
            along_x(0, i).start()
            along_y(0, 1 - i).start()

    def spread(p, i):
        along_z(p, i).wait_recv()
        pl.when(inner)(block_pass(p, i).start)
        along_x(p, i).start()
        along_y(p, i).start()

    started.append(corner_z(0))
    inner_started += [corner_pass(0), corner_pass(1)]
    for p in range(4):
        for i in range(2):
            inner_started.append(block_pass(p, i))
            started += [along_x(p, i), along_y(p, i)]
        if p in through:
            started += [half_x(p), half_y(p)]
    started += [along_z(0, 0), along_z(0, 1)]

    def cross_first(p):
        along_x(p, 0).wait_recv()
        half_y(p).start()
        along_y(p, 1).wait_recv()
        half_x(p).start()

    def cross_rest(p):
        if p not in through:
            along_x(p, 0).wait_recv()
            along_y(p, 1).wait_recv()
        along_x(p, 1).wait_recv()
        along_y(p, 0).wait_recv()

    def corner(p):
        if p in through:
            half_x(p).wait_recv()
            half_y(p).wait_recv()
        else:
            corner_z(p).wait_recv()
            if p == 1:
                pl.when(inner)(corner_pass(p).start)

    per = r.got.shape[1] * r.got.shape[2]
    ff = r.wg.shape[2]
    coefs = [None] * 4

    def serve_up(p):
        g = groups[p]
        spread_w = wide(r.got[g, :, :, width:].reshape(per, LANES))
        lanes = lax.broadcasted_iota(jnp.int32, spread_w.shape, 1)
        chosen = lax.rem(lanes, LANES // 2) == sp
        coefs[p] = jnp.sum(jnp.where(chosen, spread_w, 0.0), axis=1, keepdims=True)

        @pl.loop(0, PAIR)
        def _(i):
            rows = r.got[g, :, :, 0:width].reshape(per, width)
            gate = jnp.dot(rows, r.wg[i], preferred_element_type=jnp.float32)
            up = jnp.dot(rows, r.wu[i], preferred_element_type=jnp.float32)
            gate = jnp.minimum(gate, clamp_limit)
            up = jnp.clip(up, -clamp_limit, clamp_limit)
            r.active[i] = narrow(gate * jax.nn.sigmoid(swish_alpha * gate) * (up + 1.0))

    def serve_down(p):
        step = min(width, 1024)

        @pl.loop(0, width // step)
        def _(i):
            cols = pl.ds(pl.multiple_of(i * step, step), step)
            down = jnp.dot(r.active[0], r.wd[0, :, cols], preferred_element_type=jnp.float32)
            for j in range(1, PAIR):
                down = down + jnp.dot(
                    r.active[j], r.wd[j, :, cols], preferred_element_type=jnp.float32
                )
            r.summed[p, :, :, cols] = narrow(down * coefs[p]).reshape(
                r.summed.shape[1:3] + (step,)
            )

    dx_copy, dy_copy = [None] * 4, [None] * 4
    bx_copy, by_copy = [[] for _ in range(4)], [[] for _ in range(4)]
    home = [None] * 4

    def give_x(p, i, rows):
        bx_copy[p].append(
            send(
                r.summed.at[p, xb, rows], r.x_in.at[p, rows],
                r.bx_s.at[p, i], r.bx_r.at[p, i], to_x,
            )
        )

    def give_y(p, i, rows):
        by_copy[p].append(
            send(
                r.summed.at[p, yb, rows], r.y_in.at[p, rows],
                r.by_s.at[p, i], r.by_r.at[p, i], to_y,
            )
        )

    def corner_home(p):
        return remote(
            r.summed.at[p, db], r.corner_in.at[z], r.e_s.at[p], r.e_r.at[z], to_z[p]
        )

    def fold(p):
        if p == 0:
            give_x(p, 0, top)
            give_y(p, 0, bottom)
        elif p in through:
            halves(p)
            give_x(p, 0, top)
            give_y(p, 0, bottom)
        else:
            started.append(corner_home(p))
            started[-1].start()
            give_x(p, 0, slice(None))
            give_y(p, 0, slice(None))

    def halves(p):
        dx_copy[p] = send(
            r.summed.at[p, db, top], r.dx_in.at[p], r.dx_s.at[p], r.dx_r.at[p], to_x
        )
        dy_copy[p] = send(
            r.summed.at[p, db, bottom], r.dy_in.at[p], r.dy_s.at[p], r.dy_r.at[p], to_y
        )

    def feed():
        def take(p):
            g = groups[p]
            remote(
                r.summed.at[p, db], r.corner_in.at[g], r.e_s.at[p], r.e_r.at[g], to_z[p]
            ).wait_recv()
            return wide(r.corner_in[g])

        @pl.when(inner)
        def _():
            r.summed[0, db] = narrow(wide(r.summed[0, db]) + take(1) + take(2) + take(3))

        @pl.when(outer)
        def _():
            r.summed[0, db] = narrow(wide(r.summed[0, db]) + take(1))

        halves(0)

    def join(p):
        dx_copy[p].wait_recv()
        r.summed[p, yb, top] = narrow(wide(r.summed[p, yb, top]) + wide(r.dx_in[p]))
        give_y(p, 1, top)
        dy_copy[p].wait_recv()
        r.summed[p, xb, bottom] = narrow(wide(r.summed[p, xb, bottom]) + wide(r.dy_in[p]))
        give_x(p, 1, bottom)

    def gather(p):
        for copy in bx_copy[p] + by_copy[p]:
            copy.wait_recv()
        return wide(r.summed[p, mine]) + wide(r.x_in[p]) + wide(r.y_in[p])

    def leave(p):
        r.home_out[p] = narrow(gather(p))
        home[p] = send(
            r.home_out.at[p], r.home_in.at[z], r.b_s.at[p], r.b_r.at[z], to_z[p]
        )

    def corner_out():
        corner_z(0).start()
        pl.when(inner)(corner_pass(0).start)

    def on_inner(action, *args):
        pl.when(inner)(functools.partial(action, *args))

    def on_outer(action, *args):
        pl.when(outer)(functools.partial(action, *args))

    with jax.named_scope("spread"):
        begin()
        cross_first(0)
        spread(1, 0)
        on_inner(spread, 2, 0)
        cross_rest(0)
        spread(1, 1)
        on_inner(spread, 2, 1)
        corner(0)
        on_outer(corner_out)
        on_inner(spread, 3, 0)
        on_inner(spread, 3, 1)
        on_inner(corner_out)
        on_outer(spread, 2, 0)
        on_outer(spread, 2, 1)
    for copy in shared:
        copy.wait_recv()
    with jax.named_scope("serve"):
        serve_up(0)
        serve_down(0)
        on_outer(spread, 3, 0)
        on_outer(spread, 3, 1)
        fold(0)
        cross_rest(1)
        cross_rest(2)
        corner(1)
        serve_up(1)
        cross_first(3)
        serve_down(1)
        fold(1)
        cross_rest(3)
        corner(2)
        serve_up(2)
        serve_down(2)
        fold(2)
        corner(3)
        serve_up(3)
        leave(1)
        serve_down(3)
        fold(3)
        leave(2)
        join(3)
        feed()
        leave(3)
        join(0)
        mixture = gather(0)
    with jax.named_scope("back"):
        for p in range(1, 4):
            g = groups[p]
            pltpu.make_async_remote_copy(
                src_ref=r.home_out.at[p], dst_ref=r.home_in.at[g], send_sem=r.b_s.at[p],
                recv_sem=r.b_r.at[g], device_id=to_z[p], device_id_type=MESH,
            ).wait_recv()
            mixture = mixture + wide(r.home_in[g])
        r.out[...] = (r.middle[...] + scale_rows(mixture, r.gain_moe[...])).astype(r.out.dtype)
        for copy in started:
            copy.wait_send()

        @pl.when(inner)
        def _():
            for copy in inner_started:
                copy.wait_send()


def whole_layer(
    queries, keys, values, q_gain, k_gain, w_out, residual, gain_mix, gain_pre, routes,
    route_weights, w_gate, w_up, w_down, gain_moe,
):
    tokens, heads, size = queries.shape
    kv_cols = keys.shape[1] * size
    tok, width = residual.shape
    ff = w_gate.shape[1]
    full = width + LANES
    blocks = PAIR * PAIR
    half = tok // 2
    pieces = 4
    bf, f32 = jnp.bfloat16, jnp.float32
    dma = pltpu.SemaphoreType.DMA
    here = pl.BlockSpec(memory_space=pltpu.VMEM)
    there = pl.BlockSpec(memory_space=pl.ANY)
    scratch = {
        "kv": pltpu.VMEM((2, RING, PAIR, tokens, kv_cols), bf),
        "query": pltpu.VMEM((tokens * heads, kv_cols), bf),
        "top": pltpu.VMEM((tokens * heads, size), f32),
        "total": pltpu.VMEM((tokens * heads, size), f32),
        "mixed": pltpu.VMEM((tokens * heads, size), f32),
        "heads": pltpu.VMEM((tokens, heads * size), bf),
        "wo": pltpu.VMEM((heads * size, width), bf),
        "part": pltpu.VMEM((PAIR, PAIR, tok, width), bf),
        "wg": pltpu.VMEM((PAIR, width, ff), bf),
        "wu": pltpu.VMEM((PAIR, width, ff), bf),
        "wd": pltpu.VMEM((PAIR, ff, width), bf),
        "pc_in": pltpu.VMEM((PAIR, tok, width), bf),
        "py_out": pltpu.VMEM((tok, width), bf),
        "py_in": pltpu.VMEM((tok, width), bf),
        "got": pltpu.VMEM((RING, blocks, tok, full), bf),
        "middle": pltpu.VMEM((tok, width), f32),
        "active": pltpu.VMEM((PAIR, blocks * tok, ff), bf),
        "summed": pltpu.VMEM((RING, blocks, tok, width), bf),
        "dx_in": pltpu.VMEM((RING, half, width), bf),
        "dy_in": pltpu.VMEM((RING, half, width), bf),
        "x_in": pltpu.VMEM((RING, tok, width), bf),
        "corner_in": pltpu.VMEM((RING, tok, width), bf),
        "y_in": pltpu.VMEM((RING, tok, width), bf),
        "home_out": pltpu.VMEM((RING, tok, width), bf),
        "home_in": pltpu.VMEM((RING, tok, width), bf),
        "w_sem": dma((4,)),
    }
    for name, dims in (
        ("kz", (4, 2)), ("kx", (4, 2)), ("kf", (4, 2)), ("pc", (pieces,)), ("py", (pieces,)), ("z", (4, 2)), ("x", (4, 2)), ("y", (4, 2)), ("zf", (4, 2)), ("d", (4,)), ("df", (4,)), ("e", (4,)), ("hx", (4,)),
        ("hy", (4,)), ("w", (3,)), ("dx", (4,)), ("dy", (4,)), ("bx", (4, 2)),
        ("by", (4, 2)), ("b", (4,)),
    ):
        scratch[name + "_s"] = dma(dims)
        scratch[name + "_r"] = dma(dims)
    operands = (
        "queries", "keys", "values", "q_gain", "k_gain", "residual", "gain_mix", "gain_pre",
        "gain_moe", "routes", "route_weights", "wo_hbm", "wg_hbm", "wu_hbm", "wd_hbm",
    )
    names = operands + ("out",) + tuple(scratch)
    return pl.pallas_call(
        functools.partial(layer_kernel, names),
        out_shape=jax.ShapeDtypeStruct((tok, width), bf),
        in_specs=[here] * 11 + [there] * 4,
        out_specs=here,
        scratch_shapes=list(scratch.values()),
        compiler_params=pltpu.CompilerParams(
            collective_id=1, has_side_effects=True, vmem_limit_bytes=56 << 20
        ),
        name="whole_layer",
    )(
        queries, keys, values, q_gain, k_gain, residual, gain_mix, gain_pre, gain_moe, routes,
        route_weights, w_out, w_gate, w_up, w_down,
    )


def on_device(
    queries,
    keys,
    values,
    q_gain,
    k_gain,
    w_out,
    residual,
    gain_mix,
    gain_pre,
    routes,
    route_weights,
    w_gate,
    w_up,
    w_down,
    gain_moe,
):
    local_experts = w_gate.shape[0]
    experts_all = local_experts * lax.axis_size("sp")
    tok_part, width = residual.shape
    capacity = max(2, (2 * tok_part * TOP + experts_all - 1) // experts_all)
    grid_fits = lax.axis_size("sp") == RING * PAIR and lax.axis_size("tp") == PAIR * PAIR
    if grid_fits and local_experts == 1 and capacity >= tok_part:
        return whole_layer(
            queries, keys, values, q_gain[None], k_gain[None], w_out, residual,
            gain_mix[None], gain_pre[None], routes.T, route_weights.T, w_gate[0], w_up[0],
            w_down[0], gain_moe[None],
        )
    tok_rows, head_local, head_size = queries.shape
    kv_local = keys.shape[1]
    group_size = head_local // kv_local
    positions = lax.axis_index("sp") * tok_rows + jnp.arange(tok_rows, dtype=jnp.int32)
    cosine_table, sine_table = rope_tables(positions, head_size)
    q_turned = (
        turn(scale_rows(queries.astype(jnp.float32), q_gain), cosine_table, sine_table)
        * head_size ** (-0.5)
    ).astype(jnp.bfloat16)
    k_turned = turn(scale_rows(keys.astype(jnp.float32), k_gain), cosine_table, sine_table).astype(
        jnp.bfloat16
    )
    q_grouped = q_turned.reshape(tok_rows, kv_local, group_size, head_size)
    initial = (
        jnp.full((kv_local, group_size, tok_rows), -jnp.inf, jnp.float32),
        jnp.zeros((kv_local, group_size, tok_rows), jnp.float32),
        jnp.zeros((kv_local, group_size, tok_rows, head_size), jnp.float32),
    )
    carry_state = initial
    kv_cols = kv_local * head_size
    both = gather_sp(
        jnp.concatenate(
            [k_turned.reshape(tok_rows, kv_cols), values.reshape(tok_rows, kv_cols)], axis=1
        )
    ).reshape(-1, 2 * kv_cols)
    key_piece = both[:, :kv_cols].reshape(-1, kv_local, head_size)
    value_piece = both[:, kv_cols:].reshape(-1, kv_local, head_size)
    piece_rows = key_piece.shape[0]
    block_rows = math.gcd(piece_rows, 1024)
    key_blocks = key_piece.reshape(piece_rows // block_rows, block_rows, kv_local, head_size)
    value_blocks = value_piece.reshape(piece_rows // block_rows, block_rows, kv_local, head_size)

    def absorb_block(state_now, key_value):
        running_max, running_sum, weighted = state_now
        key_block, value_block = key_value
        scores = jnp.einsum(
            "qkgd,skd->kgqs", q_grouped, key_block, preferred_element_type=jnp.float32
        )
        new_max = jnp.maximum(running_max, jnp.max(scores, axis=-1))
        rescale = jnp.exp(running_max - new_max)
        unnorm = jnp.exp(scores - new_max[..., None])
        running_sum = running_sum * rescale + jnp.sum(unnorm, axis=-1)
        weighted = weighted * rescale[..., None] + jnp.einsum(
            "kgqs,skd->kgqd",
            unnorm.astype(jnp.bfloat16),
            value_block,
            preferred_element_type=jnp.float32,
        )
        return ((new_max, running_sum, weighted), None)

    carry_state, ignored = lax.scan(absorb_block, carry_state, (key_blocks, value_blocks))
    running_max, running_sum, weighted = carry_state
    mixed_heads = (weighted / running_sum[..., None]).transpose(2, 0, 1, 3)
    mixed_heads = mixed_heads.reshape(tok_rows, head_local * head_size).astype(jnp.bfloat16)
    part = jnp.dot(mixed_heads, w_out, preferred_element_type=jnp.float32).astype(jnp.bfloat16)
    projected = lax.psum_scatter(
        part,
        "tp",
        scatter_dimension=0,
        tiled=True,
    ).astype(jnp.float32)
    middle = residual.astype(jnp.float32) + scale_rows(projected, gain_mix)
    normed = scale_rows(middle, gain_pre).astype(jnp.bfloat16)
    tables = slot_table(routes, experts_all, capacity)
    chosen = jnp.sum(tables, axis=1)
    outbound = jnp.einsum("tp,td->pd", chosen, normed, preferred_element_type=jnp.float32)
    outbound = outbound.astype(jnp.bfloat16).reshape(experts_all, capacity, width)
    arrived_rows = lax.all_gather(
        lax.all_to_all(outbound, "sp", split_axis=0, concat_axis=0, tiled=True),
        "tp",
        axis=0,
        tiled=True,
    )
    leading = arrived_rows.shape[0] // local_experts
    partial_value = expert_apply(
        arrived_rows.reshape(leading, local_experts, arrived_rows.shape[1], width),
        w_gate,
        w_up,
        w_down,
    )
    summed = lax.psum_scatter(
        partial_value.reshape(arrived_rows.shape).astype(jnp.bfloat16),
        "tp",
        scatter_dimension=0,
        tiled=True,
    )
    returned = send_back(summed)
    gathered = jnp.einsum(
        "tkp,pd->tkd",
        tables,
        returned.reshape(experts_all * capacity, width),
        preferred_element_type=jnp.float32,
    )
    mixture = jnp.sum(gathered * route_weights[:, :, None], axis=1)
    return (middle + scale_rows(mixture, gain_moe)).astype(jnp.bfloat16)


def solution(mesh):
    placed = (
        P("sp", "tp", None),
        P("sp", "tp", None),
        P("sp", "tp", None),
        P(),
        P(),
        P("tp", None),
        P(("sp", "tp"), None),
        P(),
        P(),
        P(("sp", "tp"), None),
        P(("sp", "tp"), None),
        P("sp", None, "tp"),
        P("sp", None, "tp"),
        P("sp", "tp", None),
        P(),
    )
    return jax.shard_map(
        on_device, mesh=mesh, in_specs=placed, out_specs=P(("sp", "tp"), None), check_vma=False
    )
```

```python
import functools
import math
from types import SimpleNamespace

import jax
import jax.numpy as jnp
from jax import lax
from jax.experimental import pallas as pl
from jax.experimental.pallas import tpu as pltpu
from jax.sharding import PartitionSpec as P

TOP = 4
GRID_W = 64


norm_eps = 1e-06
rope_theta = 10000.0
clamp_limit = 7.0
swish_alpha = 1.702


def rope_tables(positions, head_size):
    row_index = (positions // GRID_W).astype(jnp.float32)
    col_index = (positions % GRID_W).astype(jnp.float32)
    freq_count = head_size // 4
    inverse = rope_theta ** (-jnp.arange(freq_count, dtype=jnp.float32) / freq_count)
    angles = jnp.stack([row_index[:, None] * inverse, col_index[:, None] * inverse], axis=1)
    return (jnp.cos(angles), jnp.sin(angles))


def turn(array_in, cosine_table, sine_table):
    token_count, head_count, head_size = array_in.shape
    split_field = array_in.reshape(token_count, head_count, 2, 2, head_size // 4)
    first_half = split_field[:, :, :, 0, :]
    second_half = split_field[:, :, :, 1, :]
    cos_wide = cosine_table[:, None]
    sin_wide = sine_table[:, None]
    turned = jnp.stack(
        [
            first_half * cos_wide - second_half * sin_wide,
            second_half * cos_wide + first_half * sin_wide,
        ],
        axis=3,
    )
    return turned.reshape(token_count, head_count, head_size)


def scale_rows(array_in, gain_vec):
    return (
        array_in
        * lax.rsqrt(jnp.mean(array_in * array_in, axis=-1, keepdims=True) + norm_eps)
        * gain_vec
    )


def slot_table(route_rows, experts, capacity):
    flat_routes = route_rows.reshape(-1)
    expert_hits = (flat_routes[:, None] == jnp.arange(experts, dtype=jnp.int32)[None, :]).astype(
        jnp.int32
    )
    slot_index = jnp.sum((jnp.cumsum(expert_hits, axis=0) - expert_hits) * expert_hits, axis=1)
    target = flat_routes * capacity + slot_index
    slot_onehot = target[:, None] == jnp.arange(experts * capacity, dtype=jnp.int32)[None, :]
    return slot_onehot.astype(jnp.bfloat16).reshape(
        route_rows.shape[0], route_rows.shape[1], experts * capacity
    )


def expert_apply(arrived_rows, w_gate, w_up, w_down):
    gate_pre = jnp.minimum(
        jnp.einsum("serd,edf->serf", arrived_rows, w_gate, preferred_element_type=jnp.float32),
        clamp_limit,
    )
    up_pre = jnp.clip(
        jnp.einsum("serd,edf->serf", arrived_rows, w_up, preferred_element_type=jnp.float32),
        -clamp_limit,
        clamp_limit,
    )
    active = (gate_pre * jax.nn.sigmoid(swish_alpha * gate_pre) * (up_pre + 1.0)).astype(
        jnp.bfloat16
    )
    partial_value = jnp.einsum("serf,efd->serd", active, w_down, preferred_element_type=jnp.float32)
    return lax.optimization_barrier(partial_value.astype(jnp.bfloat16)).astype(jnp.float32)


def send_back(finished):
    return lax.all_to_all(finished, "sp", split_axis=0, concat_axis=0, tiled=True)


MESH = pl.DeviceIdType.MESH
RING = 4
PAIR = 2
LANES = 128


def gather_kernel(n, own_ref, out_ref, send_sem, recv_sem, pass_sem, take_sem, own_sem):
    me = lax.axis_index("sp")
    tp = lax.axis_index("tp")
    pair = me + 1 - 2 * lax.rem(me, 2)
    barrier = pltpu.get_barrier_semaphore()

    def greet(i, carry):
        pl.semaphore_signal(
            barrier, inc=1, device_id=(lax.rem(me + 2 * i, n), tp), device_id_type=MESH
        )
        return carry

    lax.fori_loop(1, n // 2, greet, 0)
    pl.semaphore_signal(barrier, inc=1, device_id=(pair, tp), device_id_type=MESH)
    keep = pltpu.make_async_copy(own_ref, out_ref.at[me], own_sem)
    keep.start()
    pl.semaphore_wait(barrier, n // 2)

    def along(i):
        return pltpu.make_async_remote_copy(
            src_ref=own_ref,
            dst_ref=out_ref.at[me],
            send_sem=send_sem.at[i],
            recv_sem=recv_sem.at[i],
            device_id=(lax.rem(me + 2 * i, n), tp),
            device_id_type=MESH,
        )

    def across(i, src):
        return pltpu.make_async_remote_copy(
            src_ref=src,
            dst_ref=out_ref.at[lax.rem(me + n - 2 * i, n)],
            send_sem=pass_sem.at[i],
            recv_sem=take_sem.at[i],
            device_id=(pair, tp),
            device_id_type=MESH,
        )

    def relay(i):
        return across(i, out_ref.at[lax.rem(me + n - 2 * i, n)])

    def start(i, carry):
        along(i).start()
        return carry

    def forward(i, carry):
        along(i).wait_recv()
        relay(i).start()
        return carry

    def finish(i, carry):
        along(i).wait_send()
        relay(i).wait()
        return carry

    lax.fori_loop(1, n // 2, start, 0)
    across(0, own_ref).start()
    keep.wait()
    lax.fori_loop(1, n // 2, forward, 0)
    across(0, own_ref).wait()
    lax.fori_loop(1, n // 2, finish, 0)


def gather_sp(block):
    n = lax.axis_size("sp")
    return pl.pallas_call(
        functools.partial(gather_kernel, n),
        out_shape=jax.ShapeDtypeStruct((n,) + block.shape, block.dtype),
        in_specs=[pl.BlockSpec(memory_space=pltpu.VMEM)],
        out_specs=pl.BlockSpec(memory_space=pltpu.VMEM),
        scratch_shapes=[
            pltpu.SemaphoreType.DMA((n // 2,)),
            pltpu.SemaphoreType.DMA((n // 2,)),
            pltpu.SemaphoreType.DMA((n // 2,)),
            pltpu.SemaphoreType.DMA((n // 2,)),
            pltpu.SemaphoreType.DMA,
        ],
        compiler_params=pltpu.CompilerParams(collective_id=0, has_side_effects=True),
        cost_estimate=pl.CostEstimate(flops=0, bytes_accessed=1 << 24, transcendentals=0),
        name="gather_kv",
    )(block)


def wide(value):
    return value.astype(jnp.float32)


def layer_kernel(names, *refs):
    r = SimpleNamespace(**dict(zip(names, refs)))
    sp = lax.axis_index("sp")
    tp = lax.axis_index("tp")
    z, x = sp // PAIR, lax.rem(sp, PAIR)
    y, c = tp // PAIR, lax.rem(tp, PAIR)
    ox, oy, oc = 1 - x, 1 - y, 1 - c
    width = r.residual.shape[1]
    half = r.residual.shape[0] // 2
    top, bottom = pl.ds(0, half), pl.ds(half, half)
    upper = z // 2
    folded = z + upper * (RING - 1 - 2 * z)

    def plane(o):
        return o + upper * (RING - 1 - 2 * o)

    groups = (z, plane(folded + 1), plane(2 - 2 * folded), plane(RING - 1))
    to_c = (sp, y * PAIR + oc)
    to_y = (sp, oy * PAIR + c)
    to_x = (z * PAIR + ox, tp)
    to_z = [None] + [(g * PAIR + x, tp) for g in groups[1:]]
    peers = [to_c, to_y, to_x] + to_z[1:]
    mine, xb, yb, db = x * PAIR + y, ox * PAIR + y, x * PAIR + oy, ox * PAIR + oy

    loads = [
        pltpu.make_async_copy(a, b, r.w_sem.at[i])
        for i, (a, b) in enumerate(
            (
                (r.wg_hbm, r.wg.at[0]),
                (r.wu_hbm, r.wu.at[0]),
                (r.wd_hbm, r.wd.at[0]),
                (r.wo_hbm, r.wo),
            )
        )
    ]
    small = [
        pltpu.make_async_copy(a, b, r.q_sem.at[i])
        for i, (a, b) in enumerate(
            (
                (r.queries_hbm, r.queries),
                (r.residual_hbm, r.residual),
                (r.mix_hbm, r.gain_mix),
                (r.pre_hbm, r.gain_pre),
                (r.moe_hbm, r.gain_moe),
            )
        )
    ]
    for load in small + loads:
        load.start()
    barrier = pltpu.get_barrier_semaphore()
    for peer in peers:
        pl.semaphore_signal(barrier, inc=1, device_id=peer, device_id_type=MESH)

    started, inner_started = [], []
    inner = lax.rem(z + 1, RING) > 1
    outer = lax.rem(z + 1, RING) <= 1

    def remote(src, dst, s, t, to):
        return pltpu.make_async_remote_copy(
            src_ref=src, dst_ref=dst, send_sem=s, recv_sem=t, device_id=to, device_id_type=MESH
        )

    def send(src, dst, s, t, to):
        copy = remote(src, dst, s, t, to)
        copy.start()
        started.append(copy)
        return copy

    def passing(ref, s, t, p):
        return remote(ref, ref, s, t, to_z[1] if p == 2 else to_z[2])

    def narrow(value):
        return value.astype(jnp.bfloat16)

    tokens, heads, size = r.queries.shape
    kv_heads = r.keys.shape[1]
    kv_cols = kv_heads * size
    lane = lax.broadcasted_iota(jnp.int32, (tokens, size), 1)
    place = sp * tokens + lax.broadcasted_iota(jnp.int32, (tokens, size), 0)
    shift = GRID_W.bit_length() - 1
    quarter = size // 4
    index = jnp.where(lane < size // 2, lax.shift_right_logical(place, shift), place & (GRID_W - 1))
    freq = wide(lane & (quarter - 1))
    angle = wide(index) * jnp.exp(freq * (-math.log(rope_theta) / quarter))
    lower = (lane & quarter) == 0
    cosine = jnp.cos(angle)
    sine = jnp.where(lower, -jnp.sin(angle), jnp.sin(angle))

    def turned(value, gain):
        value = scale_rows(wide(value), gain)
        ahead = pltpu.roll(value, size - quarter, axis=value.ndim - 1)
        behind = pltpu.roll(value, quarter, axis=value.ndim - 1)
        if value.ndim == 2:
            return value * cosine + jnp.where(lower, ahead, behind) * sine
        low = (lax.broadcasted_iota(jnp.int32, value.shape, 2) & quarter) == 0
        return value * cosine[:, None] + jnp.where(low, ahead, behind) * sine[:, None]

    spans = [pl.ds(g * size, size) for g in range(kv_heads)]
    for g, cols in enumerate(spans):
        r.kv[1, z, x, :, cols] = r.values[:, g, :]
    pl.semaphore_wait(barrier, len(peers))

    def kv_at(p, i):
        return r.kv.at[i, groups[p], x]

    def kv_x(p, i):
        return remote(kv_at(p, i), kv_at(p, i), r.kx_s.at[p, i], r.kx_r.at[p, i], to_x)

    def kv_z(p, i, to):
        return remote(
            kv_at(p, i), kv_at(p, i), r.kz_s.at[p, i], r.kz_r.at[groups[p], i], to
        )

    def kv_pass(p, i):
        return passing(kv_at(p, i), r.kf_s.at[p, i], r.kz_r.at[groups[p], i], p)

    def kv_across(p, i):
        kv_z(p, i, to_z[1]).wait_recv()
        pl.when(inner)(kv_pass(p, i).start)
        if p != 2 or i == 0:
            kv_x(p, i).start()
        else:
            pl.when(outer)(kv_x(p, i).start)
        if p == 2 and i == 0:
            pl.when(inner)(kv_x(p, 1).start)

    def kv_begin(i):
        kv_z(0, i, to_z[1]).start()
        pl.when(inner)(kv_pass(0, i).start)
        kv_x(0, i).start()
        started.append(kv_z(0, i, to_z[1]))
        started.extend(kv_x(p, i) for p in range(4))
        inner_started.extend(kv_pass(p, i) for p in range(4))

    kv_begin(1)
    with jax.named_scope("keys"):
        for g, cols in enumerate(spans):
            r.kv[0, z, x, :, cols] = narrow(turned(r.keys[:, g, :], r.k_gain[...]))
    kv_begin(0)
    with jax.named_scope("queries"):
        small[0].wait()
        query = turned(r.queries[...], r.q_gain[...]) * size ** (-0.5)
        group_size = heads // kv_heads
        owner = lax.broadcasted_iota(jnp.int32, query.shape, 1) // group_size
        for g in range(kv_heads):
            r.query[:, pl.ds(g * size, size)] = narrow(
                jnp.where(owner == g, query, 0.0).reshape(tokens * heads, size)
            )
    tok = r.residual.shape[0]
    named = lax.broadcasted_iota(jnp.int32, (RING * PAIR, tok), 0)
    coef = jnp.zeros(named.shape, jnp.float32)
    for k in range(r.routes.shape[0]):
        hit = r.routes[k:k + 1, :] == named
        coef = coef + jnp.where(hit, r.route_weights[k:k + 1, :], 0.0)
    coef = jnp.concatenate(
        [coef, jnp.zeros((RING * PAIR, LANES - tok), jnp.float32)], axis=1
    )
    for e in range(RING * PAIR):
        r.rates[z, mine, e] = coef[e:e + 1, :]

    def rates_z(p):
        ref = r.rates.at[z, mine]
        return remote(ref, ref, r.az_s.at[p], r.az_r.at[z], to_z[p])

    def rates_from(p):
        ref = r.rates.at[groups[p], mine]
        return remote(ref, ref, r.az_s.at[p], r.az_r.at[groups[p]], to_z[p])

    rates_x = remote(
        r.rates.at[:, mine], r.rates.at[:, mine], r.ax_s.at[0], r.ax_r.at[0], to_x
    )
    rates_y = [
        remote(r.rates.at[:, k], r.rates.at[:, k], r.ay_s.at[i], r.ay_r.at[i], to_y)
        for i, k in enumerate((mine, xb))
    ]
    started += [rates_z(1), rates_z(2), rates_z(3), rates_x] + rates_y
    row_step = min(tokens * heads, 256)

    def attend(p, part):
        if part != 1:
            for i in range(2):
                kv_x(p, i).wait_recv()
        steps = tokens * heads // row_step
        span = {0: (0, steps // 2), 1: (steps // 2, steps), 2: (0, steps)}[part]

        @pl.loop(*span, unroll=True)
        def _(i):
            rows = pl.ds(pl.multiple_of(i * row_step, row_step), row_step)
            key = r.kv[0, groups[p]].reshape(PAIR * tokens, kv_cols)
            value = r.kv[1, groups[p]].reshape(PAIR * tokens, kv_cols)
            scores = lax.dot_general(
                r.query[rows, :], key, (((1,), (1,)), ((), ())),
                preferred_element_type=jnp.float32,
            )
            top_now = jnp.max(scores, axis=1, keepdims=True)
            if p:
                before = r.top[rows, :]
                top_now = jnp.maximum(before[:, :1], top_now)
            unnormed = jnp.exp(scores - top_now)
            total = jnp.sum(unnormed, axis=1, keepdims=True)
            both = jnp.dot(narrow(unnormed), value, preferred_element_type=jnp.float32)
            head = lax.rem(lax.broadcasted_iota(jnp.int32, (row_step, size), 0), heads)
            mixed = both[:, :size]
            for g in range(1, kv_heads):
                mixed = jnp.where(
                    head // group_size == g, both[:, g * size:(g + 1) * size], mixed
                )
            if p:
                rescale = jnp.exp(before - top_now)
                total = r.total[rows, :] * rescale + total
                mixed = r.mixed[rows, :] * rescale + mixed
            if p < 3:
                r.top[rows, :] = jnp.broadcast_to(top_now, (row_step, size))
                r.total[rows, :] = jnp.broadcast_to(total, (row_step, size))
                r.mixed[rows, :] = mixed
            else:
                r.mixed[rows, :] = mixed / total

    shared = []

    def share(i):
        ref = (r.wg, r.wu, r.wd)[i]
        loads[i].wait()
        shared.append(send(ref.at[0], ref.at[1], r.w_s.at[i], r.w_r.at[i], to_c))

    with jax.named_scope("attend"):
        for i in (1, 0):
            kv_across(1, i)
            pl.when(inner)(functools.partial(kv_across, 2, i))
        share(0)
        share(1)
        attend(0, 0)
        share(2)
        for p in range(1, 4):
            rates_z(p).start()
        pl.when(outer)(functools.partial(kv_across, 2, 1))
        pl.when(inner)(functools.partial(kv_across, 3, 1))
        attend(0, 1)
        pl.when(outer)(functools.partial(kv_across, 2, 0))
        pl.when(inner)(functools.partial(kv_across, 3, 0))
        pl.when(outer)(functools.partial(kv_across, 3, 1))
        attend(1, 0)
        pl.when(outer)(functools.partial(kv_across, 3, 0))
        attend(1, 1)
        for p in range(1, 4):
            rates_from(p).wait_recv()
        rates_x.start()
        attend(2, 2)
        attend(3, 2)
        rates_x.wait_recv()
        for copy in rates_y:
            copy.start()
        for h in range(heads):
            r.heads[:, pl.ds(h * size, size)] = narrow(
                r.mixed[pl.ds(h, tokens, stride=heads), :]
            )
    loads[3].wait()
    tok = r.residual.shape[0]
    pieces = r.pc_s.shape[0]
    piece = width // pieces
    pair_copy, y_part = [], []
    def fold_pair(i):
        cols = pl.ds(i * piece, piece)
        pair_copy[i].wait_recv()
        r.py_out[:, cols] = narrow(wide(r.part[oy, c, :, cols]) + wide(r.pc_in[oy, :, cols]))
        y_part.append(
            send(r.py_out.at[:, cols], r.py_in.at[:, cols], r.py_s.at[i], r.py_r.at[i], to_y)
        )

    with jax.named_scope("proj"):
        for i in range(pieces):
            cols = pl.ds(i * piece, piece)
            part = jnp.dot(r.heads[...], r.wo[:, cols], preferred_element_type=jnp.float32)
            r.part[:, :, :, cols] = narrow(part).reshape(PAIR, PAIR, tok, piece)
            pair_copy.append(
                send(
                    r.part.at[:, oc, :, cols], r.pc_in.at[:, :, cols],
                    r.pc_s.at[i], r.pc_r.at[i], to_c,
                )
            )
            if i:
                fold_pair(i - 1)
        fold_pair(pieces - 1)
        for i in range(pieces):
            y_part[i].wait_recv()
        for load in small[1:]:
            load.wait()
        projected = wide(r.part[y, c]) + wide(r.pc_in[y]) + wide(r.py_in[...])
        mid = wide(r.residual[...]) + scale_rows(projected, r.gain_mix[...])
        r.middle[...] = mid
        r.got[z, mine] = narrow(scale_rows(mid, r.gain_pre[...]))

    def block(p, k, rows=slice(None)):
        return r.got.at[groups[p], k, rows]

    through = (0, RING - 1)

    ends = (top, bottom)

    def along_x(p, i):
        ref = block(p, mine, ends[i])
        return remote(ref, ref, r.x_s.at[p, i], r.x_r.at[p, i], to_x)

    def along_y(p, i):
        ref = block(p, mine, ends[i])
        return remote(ref, ref, r.y_s.at[p, i], r.y_r.at[p, i], to_y)

    def along_z(p, i):
        ref = block(p, mine, ends[i])
        return remote(ref, ref, r.z_s.at[p, i], r.z_r.at[groups[p], i], to_z[1])

    def block_pass(p, i):
        return passing(block(p, mine, ends[i]), r.zf_s.at[p, i], r.z_r.at[groups[p], i], p)

    def corner_z(p):
        return remote(block(p, db), block(p, db), r.d_s.at[p], r.d_r.at[groups[p]], to_z[1])

    def corner_pass(p):
        return passing(block(p, db), r.df_s.at[p], r.d_r.at[groups[p]], p)

    def half_x(p):
        ref = block(p, yb, bottom)
        return remote(ref, ref, r.hx_s.at[p], r.hx_r.at[p], to_x)

    def half_y(p):
        ref = block(p, xb, top)
        return remote(ref, ref, r.hy_s.at[p], r.hy_r.at[p], to_y)

    def begin():
        for i in range(2):
            along_z(0, i).start()
            pl.when(inner)(block_pass(0, i).start)
            along_x(0, i).start()
            along_y(0, 1 - i).start()

    def spread(p, i):
        along_z(p, i).wait_recv()
        pl.when(inner)(block_pass(p, i).start)
        along_x(p, i).start()
        along_y(p, i).start()

    started.append(corner_z(0))
    inner_started += [corner_pass(0), corner_pass(1)]
    for p in range(4):
        for i in range(2):
            inner_started.append(block_pass(p, i))
            started += [along_x(p, i), along_y(p, i)]
        if p in through:
            started += [half_x(p), half_y(p)]
    started += [along_z(0, 0), along_z(0, 1)]

    def cross_first(p):
        along_x(p, 0).wait_recv()
        half_y(p).start()
        along_y(p, 1).wait_recv()
        half_x(p).start()

    def cross_rest(p):
        if p not in through:
            along_x(p, 0).wait_recv()
            along_y(p, 1).wait_recv()
        along_x(p, 1).wait_recv()
        along_y(p, 0).wait_recv()

    def corner(p):
        if p in through:
            half_x(p).wait_recv()
            half_y(p).wait_recv()
        else:
            corner_z(p).wait_recv()
            if p == 1:
                pl.when(inner)(corner_pass(p).start)

    per = r.got.shape[1] * r.got.shape[2]
    ff = r.wg.shape[2]
    coefs = [None] * 4

    def serve_up(p):
        g = groups[p]
        shape = (r.got.shape[1], tok, LANES)
        lanes = lax.broadcasted_iota(jnp.int32, shape, 2)
        chosen = lanes == lax.broadcasted_iota(jnp.int32, shape, 1)
        rates = jnp.where(chosen, jnp.broadcast_to(r.rates[g, :, sp], shape), 0.0)
        coefs[p] = jnp.sum(rates.reshape(per, LANES), axis=1, keepdims=True)

        @pl.loop(0, PAIR)
        def _(i):
            rows = r.got[g].reshape(per, width)
            gate = jnp.dot(rows, r.wg[i], preferred_element_type=jnp.float32)
            up = jnp.dot(rows, r.wu[i], preferred_element_type=jnp.float32)
            gate = jnp.minimum(gate, clamp_limit)
            up = jnp.clip(up, -clamp_limit, clamp_limit)
            r.active[i] = narrow(gate * jax.nn.sigmoid(swish_alpha * gate) * (up + 1.0))

    def serve_down(p):
        step = min(width, 1024)

        @pl.loop(0, width // step)
        def _(i):
            cols = pl.ds(pl.multiple_of(i * step, step), step)
            down = jnp.dot(r.active[0], r.wd[0, :, cols], preferred_element_type=jnp.float32)
            for j in range(1, PAIR):
                down = down + jnp.dot(
                    r.active[j], r.wd[j, :, cols], preferred_element_type=jnp.float32
                )
            r.summed[p, :, :, cols] = narrow(down * coefs[p]).reshape(
                r.summed.shape[1:3] + (step,)
            )

    dx_copy, dy_copy = [None] * 4, [None] * 4
    bx_copy, by_copy = [[] for _ in range(4)], [[] for _ in range(4)]
    home = [None] * 4

    def give_x(p, i, rows):
        bx_copy[p].append(
            send(
                r.summed.at[p, xb, rows], r.x_in.at[p, rows],
                r.bx_s.at[p, i], r.bx_r.at[p, i], to_x,
            )
        )

    def give_y(p, i, rows):
        by_copy[p].append(
            send(
                r.summed.at[p, yb, rows], r.y_in.at[p, rows],
                r.by_s.at[p, i], r.by_r.at[p, i], to_y,
            )
        )

    def corner_home(p):
        return remote(
            r.summed.at[p, db], r.corner_in.at[z], r.e_s.at[p], r.e_r.at[z], to_z[p]
        )

    def fold(p):
        if p == 0:
            give_x(p, 0, top)
            give_y(p, 0, bottom)
        elif p in through:
            halves(p)
            give_x(p, 0, top)
            give_y(p, 0, bottom)
        else:
            started.append(corner_home(p))
            started[-1].start()
            give_x(p, 0, slice(None))
            give_y(p, 0, slice(None))

    def halves(p):
        dx_copy[p] = send(
            r.summed.at[p, db, top], r.dx_in.at[p], r.dx_s.at[p], r.dx_r.at[p], to_x
        )
        dy_copy[p] = send(
            r.summed.at[p, db, bottom], r.dy_in.at[p], r.dy_s.at[p], r.dy_r.at[p], to_y
        )

    def feed():
        def take(p):
            g = groups[p]
            remote(
                r.summed.at[p, db], r.corner_in.at[g], r.e_s.at[p], r.e_r.at[g], to_z[p]
            ).wait_recv()
            return wide(r.corner_in[g])

        @pl.when(inner)
        def _():
            r.summed[0, db] = narrow(wide(r.summed[0, db]) + take(1) + take(2) + take(3))

        @pl.when(outer)
        def _():
            r.summed[0, db] = narrow(wide(r.summed[0, db]) + take(1))

        halves(0)

    def join(p):
        dx_copy[p].wait_recv()
        r.summed[p, yb, top] = narrow(wide(r.summed[p, yb, top]) + wide(r.dx_in[p]))
        give_y(p, 1, top)
        dy_copy[p].wait_recv()
        r.summed[p, xb, bottom] = narrow(wide(r.summed[p, xb, bottom]) + wide(r.dy_in[p]))
        give_x(p, 1, bottom)

    def gather(p):
        for copy in bx_copy[p] + by_copy[p]:
            copy.wait_recv()
        return wide(r.summed[p, mine]) + wide(r.x_in[p]) + wide(r.y_in[p])

    def leave(p):
        r.home_out[p] = narrow(gather(p))
        home[p] = send(
            r.home_out.at[p], r.home_in.at[z], r.b_s.at[p], r.b_r.at[z], to_z[p]
        )

    def corner_out():
        corner_z(0).start()
        pl.when(inner)(corner_pass(0).start)

    def on_inner(action, *args):
        pl.when(inner)(functools.partial(action, *args))

    def on_outer(action, *args):
        pl.when(outer)(functools.partial(action, *args))

    with jax.named_scope("spread"):
        begin()
        cross_first(0)
        spread(1, 0)
        on_inner(spread, 2, 0)
        cross_rest(0)
        spread(1, 1)
        on_inner(spread, 2, 1)
        corner(0)
        on_outer(corner_out)
        on_inner(spread, 3, 0)
        on_inner(spread, 3, 1)
        on_inner(corner_out)
        on_outer(spread, 2, 0)
        on_outer(spread, 2, 1)
    for copy in shared:
        copy.wait_recv()
    for copy in rates_y:
        copy.wait_recv()
    with jax.named_scope("serve"):
        serve_up(0)
        serve_down(0)
        on_outer(spread, 3, 0)
        on_outer(spread, 3, 1)
        fold(0)
        cross_rest(1)
        corner(1)
        cross_first(3)
        serve_up(1)
        serve_down(1)
        fold(1)
        cross_rest(2)
        corner(2)
        serve_up(2)
        serve_down(2)
        fold(2)
        cross_rest(3)
        corner(3)
        serve_up(3)
        serve_down(3)
        fold(3)
        leave(1)
        leave(2)
        join(3)
        feed()
        leave(3)
        join(0)
        mixture = gather(0)
    with jax.named_scope("back"):
        for p in range(1, 4):
            g = groups[p]
            pltpu.make_async_remote_copy(
                src_ref=r.home_out.at[p], dst_ref=r.home_in.at[g], send_sem=r.b_s.at[p],
                recv_sem=r.b_r.at[g], device_id=to_z[p], device_id_type=MESH,
            ).wait_recv()
            mixture = mixture + wide(r.home_in[g])
        r.out[...] = (r.middle[...] + scale_rows(mixture, r.gain_moe[...])).astype(r.out.dtype)
        for copy in started:
            copy.wait_send()

        @pl.when(inner)
        def _():
            for copy in inner_started:
                copy.wait_send()


def whole_layer(
    queries, keys, values, q_gain, k_gain, w_out, residual, gain_mix, gain_pre, routes,
    route_weights, w_gate, w_up, w_down, gain_moe,
):
    tokens, heads, size = queries.shape
    kv_cols = keys.shape[1] * size
    tok, width = residual.shape
    ff = w_gate.shape[1]
    blocks = PAIR * PAIR
    half = tok // 2
    pieces = 4
    bf, f32 = jnp.bfloat16, jnp.float32
    dma = pltpu.SemaphoreType.DMA
    here = pl.BlockSpec(memory_space=pltpu.VMEM)
    there = pl.BlockSpec(memory_space=pl.ANY)
    scratch = {
        "kv": pltpu.VMEM((2, RING, PAIR, tokens, kv_cols), bf),
        "query": pltpu.VMEM((tokens * heads, kv_cols), bf),
        "top": pltpu.VMEM((tokens * heads, size), f32),
        "total": pltpu.VMEM((tokens * heads, size), f32),
        "mixed": pltpu.VMEM((tokens * heads, size), f32),
        "heads": pltpu.VMEM((tokens, heads * size), bf),
        "wo": pltpu.VMEM((heads * size, width), bf),
        "part": pltpu.VMEM((PAIR, PAIR, tok, width), bf),
        "wg": pltpu.VMEM((PAIR, width, ff), bf),
        "wu": pltpu.VMEM((PAIR, width, ff), bf),
        "wd": pltpu.VMEM((PAIR, ff, width), bf),
        "pc_in": pltpu.VMEM((PAIR, tok, width), bf),
        "py_out": pltpu.VMEM((tok, width), bf),
        "py_in": pltpu.VMEM((tok, width), bf),
        "got": pltpu.VMEM((RING, blocks, tok, width), bf),
        "rates": pltpu.VMEM((RING, blocks, RING * PAIR, 1, LANES), f32),
        "middle": pltpu.VMEM((tok, width), f32),
        "active": pltpu.VMEM((PAIR, blocks * tok, ff), bf),
        "summed": pltpu.VMEM((RING, blocks, tok, width), bf),
        "dx_in": pltpu.VMEM((RING, half, width), bf),
        "dy_in": pltpu.VMEM((RING, half, width), bf),
        "x_in": pltpu.VMEM((RING, tok, width), bf),
        "corner_in": pltpu.VMEM((RING, tok, width), bf),
        "y_in": pltpu.VMEM((RING, tok, width), bf),
        "home_out": pltpu.VMEM((RING, tok, width), bf),
        "home_in": pltpu.VMEM((RING, tok, width), bf),
        "queries": pltpu.VMEM(queries.shape, bf),
        "residual": pltpu.VMEM(residual.shape, bf),
        "gain_mix": pltpu.VMEM(gain_mix.shape, f32),
        "gain_pre": pltpu.VMEM(gain_pre.shape, f32),
        "gain_moe": pltpu.VMEM(gain_moe.shape, f32),
        "q_sem": dma((5,)),
        "w_sem": dma((4,)),
    }
    for name, dims in (
        ("kz", (4, 2)), ("kx", (4, 2)), ("kf", (4, 2)), ("pc", (pieces,)), ("py", (pieces,)), ("z", (4, 2)), ("x", (4, 2)), ("y", (4, 2)), ("zf", (4, 2)), ("d", (4,)), ("df", (4,)), ("e", (4,)), ("hx", (4,)),
        ("hy", (4,)), ("w", (3,)), ("az", (4,)), ("ax", (1,)), ("ay", (2,)), ("dx", (4,)), ("dy", (4,)), ("bx", (4, 2)),
        ("by", (4, 2)), ("b", (4,)),
    ):
        scratch[name + "_s"] = dma(dims)
        scratch[name + "_r"] = dma(dims)
    operands = (
        "keys", "values", "q_gain", "k_gain", "routes", "route_weights", "queries_hbm",
        "residual_hbm", "mix_hbm", "pre_hbm", "moe_hbm", "wo_hbm", "wg_hbm", "wu_hbm", "wd_hbm",
    )
    names = operands + ("out",) + tuple(scratch)
    return pl.pallas_call(
        functools.partial(layer_kernel, names),
        out_shape=jax.ShapeDtypeStruct((tok, width), bf),
        in_specs=[here] * 6 + [there] * 9,
        out_specs=here,
        scratch_shapes=list(scratch.values()),
        compiler_params=pltpu.CompilerParams(
            collective_id=1, has_side_effects=True, vmem_limit_bytes=56 << 20
        ),
        name="whole_layer",
    )(
        keys, values, q_gain, k_gain, routes, route_weights, queries, residual, gain_mix,
        gain_pre, gain_moe, w_out, w_gate, w_up, w_down,
    )


def on_device(
    queries,
    keys,
    values,
    q_gain,
    k_gain,
    w_out,
    residual,
    gain_mix,
    gain_pre,
    routes,
    route_weights,
    w_gate,
    w_up,
    w_down,
    gain_moe,
):
    local_experts = w_gate.shape[0]
    experts_all = local_experts * lax.axis_size("sp")
    tok_part, width = residual.shape
    capacity = max(2, (2 * tok_part * TOP + experts_all - 1) // experts_all)
    grid_fits = lax.axis_size("sp") == RING * PAIR and lax.axis_size("tp") == PAIR * PAIR
    if grid_fits and local_experts == 1 and capacity >= tok_part:
        return whole_layer(
            queries, keys, values, q_gain[None], k_gain[None], w_out, residual,
            gain_mix[None], gain_pre[None], routes.T, route_weights.T, w_gate[0], w_up[0],
            w_down[0], gain_moe[None],
        )
    tok_rows, head_local, head_size = queries.shape
    kv_local = keys.shape[1]
    group_size = head_local // kv_local
    positions = lax.axis_index("sp") * tok_rows + jnp.arange(tok_rows, dtype=jnp.int32)
    cosine_table, sine_table = rope_tables(positions, head_size)
    q_turned = (
        turn(scale_rows(queries.astype(jnp.float32), q_gain), cosine_table, sine_table)
        * head_size ** (-0.5)
    ).astype(jnp.bfloat16)
    k_turned = turn(scale_rows(keys.astype(jnp.float32), k_gain), cosine_table, sine_table).astype(
        jnp.bfloat16
    )
    q_grouped = q_turned.reshape(tok_rows, kv_local, group_size, head_size)
    initial = (
        jnp.full((kv_local, group_size, tok_rows), -jnp.inf, jnp.float32),
        jnp.zeros((kv_local, group_size, tok_rows), jnp.float32),
        jnp.zeros((kv_local, group_size, tok_rows, head_size), jnp.float32),
    )
    carry_state = initial
    kv_cols = kv_local * head_size
    both = gather_sp(
        jnp.concatenate(
            [k_turned.reshape(tok_rows, kv_cols), values.reshape(tok_rows, kv_cols)], axis=1
        )
    ).reshape(-1, 2 * kv_cols)
    key_piece = both[:, :kv_cols].reshape(-1, kv_local, head_size)
    value_piece = both[:, kv_cols:].reshape(-1, kv_local, head_size)
    piece_rows = key_piece.shape[0]
    block_rows = math.gcd(piece_rows, 1024)
    key_blocks = key_piece.reshape(piece_rows // block_rows, block_rows, kv_local, head_size)
    value_blocks = value_piece.reshape(piece_rows // block_rows, block_rows, kv_local, head_size)

    def absorb_block(state_now, key_value):
        running_max, running_sum, weighted = state_now
        key_block, value_block = key_value
        scores = jnp.einsum(
            "qkgd,skd->kgqs", q_grouped, key_block, preferred_element_type=jnp.float32
        )
        new_max = jnp.maximum(running_max, jnp.max(scores, axis=-1))
        rescale = jnp.exp(running_max - new_max)
        unnorm = jnp.exp(scores - new_max[..., None])
        running_sum = running_sum * rescale + jnp.sum(unnorm, axis=-1)
        weighted = weighted * rescale[..., None] + jnp.einsum(
            "kgqs,skd->kgqd",
            unnorm.astype(jnp.bfloat16),
            value_block,
            preferred_element_type=jnp.float32,
        )
        return ((new_max, running_sum, weighted), None)

    carry_state, ignored = lax.scan(absorb_block, carry_state, (key_blocks, value_blocks))
    running_max, running_sum, weighted = carry_state
    mixed_heads = (weighted / running_sum[..., None]).transpose(2, 0, 1, 3)
    mixed_heads = mixed_heads.reshape(tok_rows, head_local * head_size).astype(jnp.bfloat16)
    part = jnp.dot(mixed_heads, w_out, preferred_element_type=jnp.float32).astype(jnp.bfloat16)
    projected = lax.psum_scatter(
        part,
        "tp",
        scatter_dimension=0,
        tiled=True,
    ).astype(jnp.float32)
    middle = residual.astype(jnp.float32) + scale_rows(projected, gain_mix)
    normed = scale_rows(middle, gain_pre).astype(jnp.bfloat16)
    tables = slot_table(routes, experts_all, capacity)
    chosen = jnp.sum(tables, axis=1)
    outbound = jnp.einsum("tp,td->pd", chosen, normed, preferred_element_type=jnp.float32)
    outbound = outbound.astype(jnp.bfloat16).reshape(experts_all, capacity, width)
    arrived_rows = lax.all_gather(
        lax.all_to_all(outbound, "sp", split_axis=0, concat_axis=0, tiled=True),
        "tp",
        axis=0,
        tiled=True,
    )
    leading = arrived_rows.shape[0] // local_experts
    partial_value = expert_apply(
        arrived_rows.reshape(leading, local_experts, arrived_rows.shape[1], width),
        w_gate,
        w_up,
        w_down,
    )
    summed = lax.psum_scatter(
        partial_value.reshape(arrived_rows.shape).astype(jnp.bfloat16),
        "tp",
        scatter_dimension=0,
        tiled=True,
    )
    returned = send_back(summed)
    gathered = jnp.einsum(
        "tkp,pd->tkd",
        tables,
        returned.reshape(experts_all * capacity, width),
        preferred_element_type=jnp.float32,
    )
    mixture = jnp.sum(gathered * route_weights[:, :, None], axis=1)
    return (middle + scale_rows(mixture, gain_moe)).astype(jnp.bfloat16)


def solution(mesh):
    placed = (
        P("sp", "tp", None),
        P("sp", "tp", None),
        P("sp", "tp", None),
        P(),
        P(),
        P("tp", None),
        P(("sp", "tp"), None),
        P(),
        P(),
        P(("sp", "tp"), None),
        P(("sp", "tp"), None),
        P("sp", None, "tp"),
        P("sp", None, "tp"),
        P("sp", "tp", None),
        P(),
    )
    return jax.shard_map(
        on_device, mesh=mesh, in_specs=placed, out_specs=P(("sp", "tp"), None), check_vma=False
    )
```

```python
import functools
import math
from types import SimpleNamespace

import jax
import jax.numpy as jnp
from jax import lax
from jax.experimental import pallas as pl
from jax.experimental.pallas import tpu as pltpu
from jax.sharding import PartitionSpec as P

TOP = 4
GRID_W = 64


norm_eps = 1e-06
rope_theta = 10000.0
clamp_limit = 7.0
swish_alpha = 1.702


def rope_tables(positions, head_size):
    row_index = (positions // GRID_W).astype(jnp.float32)
    col_index = (positions % GRID_W).astype(jnp.float32)
    freq_count = head_size // 4
    inverse = rope_theta ** (-jnp.arange(freq_count, dtype=jnp.float32) / freq_count)
    angles = jnp.stack([row_index[:, None] * inverse, col_index[:, None] * inverse], axis=1)
    return (jnp.cos(angles), jnp.sin(angles))


def turn(array_in, cosine_table, sine_table):
    token_count, head_count, head_size = array_in.shape
    split_field = array_in.reshape(token_count, head_count, 2, 2, head_size // 4)
    first_half = split_field[:, :, :, 0, :]
    second_half = split_field[:, :, :, 1, :]
    cos_wide = cosine_table[:, None]
    sin_wide = sine_table[:, None]
    turned = jnp.stack(
        [
            first_half * cos_wide - second_half * sin_wide,
            second_half * cos_wide + first_half * sin_wide,
        ],
        axis=3,
    )
    return turned.reshape(token_count, head_count, head_size)


def scale_rows(array_in, gain_vec):
    return (
        array_in
        * lax.rsqrt(jnp.mean(array_in * array_in, axis=-1, keepdims=True) + norm_eps)
        * gain_vec
    )


def slot_table(route_rows, experts, capacity):
    flat_routes = route_rows.reshape(-1)
    expert_hits = (flat_routes[:, None] == jnp.arange(experts, dtype=jnp.int32)[None, :]).astype(
        jnp.int32
    )
    slot_index = jnp.sum((jnp.cumsum(expert_hits, axis=0) - expert_hits) * expert_hits, axis=1)
    target = flat_routes * capacity + slot_index
    slot_onehot = target[:, None] == jnp.arange(experts * capacity, dtype=jnp.int32)[None, :]
    return slot_onehot.astype(jnp.bfloat16).reshape(
        route_rows.shape[0], route_rows.shape[1], experts * capacity
    )


def expert_apply(arrived_rows, w_gate, w_up, w_down):
    gate_pre = jnp.minimum(
        jnp.einsum("serd,edf->serf", arrived_rows, w_gate, preferred_element_type=jnp.float32),
        clamp_limit,
    )
    up_pre = jnp.clip(
        jnp.einsum("serd,edf->serf", arrived_rows, w_up, preferred_element_type=jnp.float32),
        -clamp_limit,
        clamp_limit,
    )
    active = (gate_pre * jax.nn.sigmoid(swish_alpha * gate_pre) * (up_pre + 1.0)).astype(
        jnp.bfloat16
    )
    partial_value = jnp.einsum("serf,efd->serd", active, w_down, preferred_element_type=jnp.float32)
    return lax.optimization_barrier(partial_value.astype(jnp.bfloat16)).astype(jnp.float32)


def send_back(finished):
    return lax.all_to_all(finished, "sp", split_axis=0, concat_axis=0, tiled=True)


MESH = pl.DeviceIdType.MESH
RING = 4
PAIR = 2
LANES = 128


def gather_kernel(n, own_ref, out_ref, send_sem, recv_sem, pass_sem, take_sem, own_sem):
    me = lax.axis_index("sp")
    tp = lax.axis_index("tp")
    pair = me + 1 - 2 * lax.rem(me, 2)
    barrier = pltpu.get_barrier_semaphore()

    def greet(i, carry):
        pl.semaphore_signal(
            barrier, inc=1, device_id=(lax.rem(me + 2 * i, n), tp), device_id_type=MESH
        )
        return carry

    lax.fori_loop(1, n // 2, greet, 0)
    pl.semaphore_signal(barrier, inc=1, device_id=(pair, tp), device_id_type=MESH)
    keep = pltpu.make_async_copy(own_ref, out_ref.at[me], own_sem)
    keep.start()
    pl.semaphore_wait(barrier, n // 2)

    def along(i):
        return pltpu.make_async_remote_copy(
            src_ref=own_ref,
            dst_ref=out_ref.at[me],
            send_sem=send_sem.at[i],
            recv_sem=recv_sem.at[i],
            device_id=(lax.rem(me + 2 * i, n), tp),
            device_id_type=MESH,
        )

    def across(i, src):
        return pltpu.make_async_remote_copy(
            src_ref=src,
            dst_ref=out_ref.at[lax.rem(me + n - 2 * i, n)],
            send_sem=pass_sem.at[i],
            recv_sem=take_sem.at[i],
            device_id=(pair, tp),
            device_id_type=MESH,
        )

    def relay(i):
        return across(i, out_ref.at[lax.rem(me + n - 2 * i, n)])

    def start(i, carry):
        along(i).start()
        return carry

    def forward(i, carry):
        along(i).wait_recv()
        relay(i).start()
        return carry

    def finish(i, carry):
        along(i).wait_send()
        relay(i).wait()
        return carry

    lax.fori_loop(1, n // 2, start, 0)
    across(0, own_ref).start()
    keep.wait()
    lax.fori_loop(1, n // 2, forward, 0)
    across(0, own_ref).wait()
    lax.fori_loop(1, n // 2, finish, 0)


def gather_sp(block):
    n = lax.axis_size("sp")
    return pl.pallas_call(
        functools.partial(gather_kernel, n),
        out_shape=jax.ShapeDtypeStruct((n,) + block.shape, block.dtype),
        in_specs=[pl.BlockSpec(memory_space=pltpu.VMEM)],
        out_specs=pl.BlockSpec(memory_space=pltpu.VMEM),
        scratch_shapes=[
            pltpu.SemaphoreType.DMA((n // 2,)),
            pltpu.SemaphoreType.DMA((n // 2,)),
            pltpu.SemaphoreType.DMA((n // 2,)),
            pltpu.SemaphoreType.DMA((n // 2,)),
            pltpu.SemaphoreType.DMA,
        ],
        compiler_params=pltpu.CompilerParams(collective_id=0, has_side_effects=True),
        cost_estimate=pl.CostEstimate(flops=0, bytes_accessed=1 << 24, transcendentals=0),
        name="gather_kv",
    )(block)


def wide(value):
    return value.astype(jnp.float32)


def layer_kernel(names, *refs):
    r = SimpleNamespace(**dict(zip(names, refs)))
    sp = lax.axis_index("sp")
    tp = lax.axis_index("tp")
    z, x = sp // PAIR, lax.rem(sp, PAIR)
    y, c = tp // PAIR, lax.rem(tp, PAIR)
    ox, oy, oc = 1 - x, 1 - y, 1 - c
    width = r.residual.shape[1]
    half = r.residual.shape[0] // 2
    top, bottom = pl.ds(0, half), pl.ds(half, half)
    upper = z // 2
    folded = z + upper * (RING - 1 - 2 * z)

    def plane(o):
        return o + upper * (RING - 1 - 2 * o)

    groups = (z, plane(folded + 1), plane(2 - 2 * folded), plane(RING - 1))
    to_c = (sp, y * PAIR + oc)
    to_y = (sp, oy * PAIR + c)
    to_x = (z * PAIR + ox, tp)
    to_z = [None] + [(g * PAIR + x, tp) for g in groups[1:]]
    peers = [to_c, to_y, to_x] + to_z[1:]
    mine, xb, yb, db = x * PAIR + y, ox * PAIR + y, x * PAIR + oy, ox * PAIR + oy

    loads = [
        pltpu.make_async_copy(a, b, r.w_sem.at[i])
        for i, (a, b) in enumerate(
            (
                (r.wg_hbm, r.wg.at[0]),
                (r.wu_hbm, r.wu.at[0]),
                (r.wd_hbm, r.wd.at[0]),
                (r.wo_hbm, r.wo),
            )
        )
    ]
    small = [
        pltpu.make_async_copy(a, b, r.q_sem.at[i])
        for i, (a, b) in enumerate(
            (
                (r.queries_hbm, r.queries),
                (r.residual_hbm, r.residual),
                (r.mix_hbm, r.gain_mix),
                (r.pre_hbm, r.gain_pre),
                (r.moe_hbm, r.gain_moe),
            )
        )
    ]
    for load in small + loads:
        load.start()
    barrier = pltpu.get_barrier_semaphore()
    for peer in peers:
        pl.semaphore_signal(barrier, inc=1, device_id=peer, device_id_type=MESH)

    started, inner_started = [], []
    inner = lax.rem(z + 1, RING) > 1
    outer = lax.rem(z + 1, RING) <= 1

    def remote(src, dst, s, t, to):
        return pltpu.make_async_remote_copy(
            src_ref=src, dst_ref=dst, send_sem=s, recv_sem=t, device_id=to, device_id_type=MESH
        )

    def send(src, dst, s, t, to):
        copy = remote(src, dst, s, t, to)
        copy.start()
        started.append(copy)
        return copy

    def passing(ref, s, t, p):
        return remote(ref, ref, s, t, to_z[1] if p == 2 else to_z[2])

    def narrow(value):
        return value.astype(jnp.bfloat16)

    tokens, heads, size = r.queries.shape
    kv_heads = r.keys.shape[1]
    kv_cols = kv_heads * size
    lane = lax.broadcasted_iota(jnp.int32, (tokens, size), 1)
    place = sp * tokens + lax.broadcasted_iota(jnp.int32, (tokens, size), 0)
    shift = GRID_W.bit_length() - 1
    quarter = size // 4
    index = jnp.where(lane < size // 2, lax.shift_right_logical(place, shift), place & (GRID_W - 1))
    freq = wide(lane & (quarter - 1))
    angle = wide(index) * jnp.exp(freq * (-math.log(rope_theta) / quarter))
    lower = (lane & quarter) == 0
    cosine = jnp.cos(angle)
    sine = jnp.where(lower, -jnp.sin(angle), jnp.sin(angle))

    def turned(value, gain):
        value = scale_rows(wide(value), gain)
        ahead = pltpu.roll(value, size - quarter, axis=value.ndim - 1)
        behind = pltpu.roll(value, quarter, axis=value.ndim - 1)
        if value.ndim == 2:
            return value * cosine + jnp.where(lower, ahead, behind) * sine
        low = (lax.broadcasted_iota(jnp.int32, value.shape, 2) & quarter) == 0
        return value * cosine[:, None] + jnp.where(low, ahead, behind) * sine[:, None]

    spans = [pl.ds(g * size, size) for g in range(kv_heads)]
    for g, cols in enumerate(spans):
        r.kv[1, z, x, :, cols] = r.values[:, g, :]
    pl.semaphore_wait(barrier, len(peers))

    def kv_at(p, i):
        return r.kv.at[i, groups[p], x]

    def kv_x(p, i):
        return remote(kv_at(p, i), kv_at(p, i), r.kx_s.at[p, i], r.kx_r.at[p, i], to_x)

    def kv_z(p, i, to):
        return remote(
            kv_at(p, i), kv_at(p, i), r.kz_s.at[p, i], r.kz_r.at[groups[p], i], to
        )

    def kv_pass(p, i):
        return passing(kv_at(p, i), r.kf_s.at[p, i], r.kz_r.at[groups[p], i], p)

    def kv_across(p, i):
        kv_z(p, i, to_z[1]).wait_recv()
        pl.when(inner)(kv_pass(p, i).start)
        if p != 2 or i == 0:
            kv_x(p, i).start()
        else:
            pl.when(outer)(kv_x(p, i).start)
        if p == 2 and i == 0:
            pl.when(inner)(kv_x(p, 1).start)

    def kv_begin(i):
        kv_z(0, i, to_z[1]).start()
        pl.when(inner)(kv_pass(0, i).start)
        kv_x(0, i).start()
        started.append(kv_z(0, i, to_z[1]))
        started.extend(kv_x(p, i) for p in range(4))
        inner_started.extend(kv_pass(p, i) for p in range(4))

    kv_begin(1)
    with jax.named_scope("keys"):
        for g, cols in enumerate(spans):
            r.kv[0, z, x, :, cols] = narrow(turned(r.keys[:, g, :], r.k_gain[...]))
    kv_begin(0)
    with jax.named_scope("queries"):
        small[0].wait()
        query = turned(r.queries[...], r.q_gain[...]) * size ** (-0.5)
        group_size = heads // kv_heads
        owner = lax.broadcasted_iota(jnp.int32, query.shape, 1) // group_size
        for g in range(kv_heads):
            r.query[:, pl.ds(g * size, size)] = narrow(
                jnp.where(owner == g, query, 0.0).reshape(tokens * heads, size)
            )
    tok = r.residual.shape[0]
    named = lax.broadcasted_iota(jnp.int32, (RING * PAIR, tok), 0)
    coef = jnp.zeros(named.shape, jnp.float32)
    for k in range(r.routes.shape[0]):
        hit = r.routes[k:k + 1, :] == named
        coef = coef + jnp.where(hit, r.route_weights[k:k + 1, :], 0.0)
    coef = jnp.concatenate(
        [coef, jnp.zeros((RING * PAIR, LANES - tok), jnp.float32)], axis=1
    )
    for e in range(RING * PAIR):
        r.rates[z, mine, e] = coef[e:e + 1, :]

    def rates_z(p):
        ref = r.rates.at[z, mine]
        return remote(ref, ref, r.az_s.at[p], r.az_r.at[z], to_z[p])

    def rates_from(p):
        ref = r.rates.at[groups[p], mine]
        return remote(ref, ref, r.az_s.at[p], r.az_r.at[groups[p]], to_z[p])

    rates_x = remote(
        r.rates.at[:, mine], r.rates.at[:, mine], r.ax_s.at[0], r.ax_r.at[0], to_x
    )
    rates_y = [
        remote(r.rates.at[:, k], r.rates.at[:, k], r.ay_s.at[i], r.ay_r.at[i], to_y)
        for i, k in enumerate((mine, xb))
    ]
    started += [rates_z(1), rates_z(2), rates_z(3), rates_x] + rates_y
    row_step = min(tokens * heads, 256)

    def attend(p, part):
        if part != 1:
            for i in range(2):
                kv_x(p, i).wait_recv()
        steps = tokens * heads // row_step
        span = {0: (0, steps // 2), 1: (steps // 2, steps), 2: (0, steps)}[part]

        @pl.loop(*span, unroll=True)
        def _(i):
            rows = pl.ds(pl.multiple_of(i * row_step, row_step), row_step)
            key = r.kv[0, groups[p]].reshape(PAIR * tokens, kv_cols)
            value = r.kv[1, groups[p]].reshape(PAIR * tokens, kv_cols)
            scores = lax.dot_general(
                r.query[rows, :], key, (((1,), (1,)), ((), ())),
                preferred_element_type=jnp.float32,
            )
            top_now = jnp.max(scores, axis=1, keepdims=True)
            if p:
                before = r.top[rows, :]
                top_now = jnp.maximum(before[:, :1], top_now)
            unnormed = jnp.exp(scores - top_now)
            total = jnp.sum(unnormed, axis=1, keepdims=True)
            both = jnp.dot(narrow(unnormed), value, preferred_element_type=jnp.float32)
            head = lax.rem(lax.broadcasted_iota(jnp.int32, (row_step, size), 0), heads)
            mixed = both[:, :size]
            for g in range(1, kv_heads):
                mixed = jnp.where(
                    head // group_size == g, both[:, g * size:(g + 1) * size], mixed
                )
            if p:
                rescale = jnp.exp(before - top_now)
                total = r.total[rows, :] * rescale + total
                mixed = r.mixed[rows, :] * rescale + mixed
            if p < 3:
                r.top[rows, :] = jnp.broadcast_to(top_now, (row_step, size))
                r.total[rows, :] = jnp.broadcast_to(total, (row_step, size))
                r.mixed[rows, :] = mixed
            else:
                r.mixed[rows, :] = mixed / total

    shared = []

    def share(i):
        ref = (r.wg, r.wu, r.wd)[i]
        loads[i].wait()
        shared.append(send(ref.at[0], ref.at[1], r.w_s.at[i], r.w_r.at[i], to_c))

    with jax.named_scope("attend"):
        for i in (1, 0):
            kv_across(1, i)
            pl.when(inner)(functools.partial(kv_across, 2, i))
        share(0)
        share(1)
        attend(0, 0)
        share(2)
        for p in range(1, 4):
            rates_z(p).start()
        pl.when(outer)(functools.partial(kv_across, 2, 1))
        pl.when(inner)(functools.partial(kv_across, 3, 1))
        attend(0, 1)
        pl.when(outer)(functools.partial(kv_across, 2, 0))
        pl.when(inner)(functools.partial(kv_across, 3, 0))
        pl.when(outer)(functools.partial(kv_across, 3, 1))
        attend(1, 0)
        pl.when(outer)(functools.partial(kv_across, 3, 0))
        attend(1, 1)
        for p in range(1, 4):
            rates_from(p).wait_recv()
        rates_x.start()
        attend(2, 2)
        attend(3, 2)
        rates_x.wait_recv()
        for copy in rates_y:
            copy.start()
        for h in range(heads):
            r.heads[:, pl.ds(h * size, size)] = narrow(
                r.mixed[pl.ds(h, tokens, stride=heads), :]
            )
    loads[3].wait()
    tok = r.residual.shape[0]
    pieces = r.pc_s.shape[0]
    piece = width // pieces
    pair_copy, y_part = [], []
    def fold_pair(i):
        cols = pl.ds(i * piece, piece)
        pair_copy[i].wait_recv()
        r.py_out[:, cols] = narrow(wide(r.part[oy, c, :, cols]) + wide(r.pc_in[oy, :, cols]))
        y_part.append(
            send(r.py_out.at[:, cols], r.py_in.at[:, cols], r.py_s.at[i], r.py_r.at[i], to_y)
        )

    with jax.named_scope("proj"):
        for i in range(pieces):
            cols = pl.ds(i * piece, piece)
            part = jnp.dot(r.heads[...], r.wo[:, cols], preferred_element_type=jnp.float32)
            r.part[:, :, :, cols] = narrow(part).reshape(PAIR, PAIR, tok, piece)
            pair_copy.append(
                send(
                    r.part.at[:, oc, :, cols], r.pc_in.at[:, :, cols],
                    r.pc_s.at[i], r.pc_r.at[i], to_c,
                )
            )
            if i:
                fold_pair(i - 1)
        fold_pair(pieces - 1)
        for i in range(pieces):
            y_part[i].wait_recv()
        for load in small[1:]:
            load.wait()
        projected = wide(r.part[y, c]) + wide(r.pc_in[y]) + wide(r.py_in[...])
        mid = wide(r.residual[...]) + scale_rows(projected, r.gain_mix[...])
        r.middle[...] = mid
        r.got[z, mine] = narrow(scale_rows(mid, r.gain_pre[...]))

    def block(p, k, rows=slice(None)):
        return r.got.at[groups[p], k, rows]

    through = (0, RING - 1)

    ends = (top, bottom)

    def along_x(p, i):
        ref = block(p, mine, ends[i])
        return remote(ref, ref, r.x_s.at[p, i], r.x_r.at[p, i], to_x)

    def along_y(p, i):
        ref = block(p, mine, ends[i])
        return remote(ref, ref, r.y_s.at[p, i], r.y_r.at[p, i], to_y)

    def along_z(p, i):
        ref = block(p, mine, ends[i])
        return remote(ref, ref, r.z_s.at[p, i], r.z_r.at[groups[p], i], to_z[1])

    def block_pass(p, i):
        return passing(block(p, mine, ends[i]), r.zf_s.at[p, i], r.z_r.at[groups[p], i], p)

    def corner_z(p):
        return remote(block(p, db), block(p, db), r.d_s.at[p], r.d_r.at[groups[p]], to_z[1])

    def corner_pass(p):
        return passing(block(p, db), r.df_s.at[p], r.d_r.at[groups[p]], p)

    def half_x(p):
        ref = block(p, yb, bottom)
        return remote(ref, ref, r.hx_s.at[p], r.hx_r.at[p], to_x)

    def half_y(p):
        ref = block(p, xb, top)
        return remote(ref, ref, r.hy_s.at[p], r.hy_r.at[p], to_y)

    def begin():
        for i in range(2):
            along_z(0, i).start()
            pl.when(inner)(block_pass(0, i).start)
            along_x(0, i).start()
            along_y(0, 1 - i).start()

    def spread(p, i):
        along_z(p, i).wait_recv()
        pl.when(inner)(block_pass(p, i).start)
        along_x(p, i).start()
        along_y(p, i).start()

    started.append(corner_z(0))
    inner_started += [corner_pass(0), corner_pass(1)]
    for p in range(4):
        for i in range(2):
            inner_started.append(block_pass(p, i))
            started += [along_x(p, i), along_y(p, i)]
        if p in through:
            started += [half_x(p), half_y(p)]
    started += [along_z(0, 0), along_z(0, 1)]

    def cross_first(p):
        along_x(p, 0).wait_recv()
        half_y(p).start()
        along_y(p, 1).wait_recv()
        half_x(p).start()

    def cross_rest(p):
        if p not in through:
            along_x(p, 0).wait_recv()
            along_y(p, 1).wait_recv()
        along_x(p, 1).wait_recv()
        along_y(p, 0).wait_recv()

    def corner(p):
        if p in through:
            half_x(p).wait_recv()
            half_y(p).wait_recv()
        else:
            corner_z(p).wait_recv()
            if p == 1:
                pl.when(inner)(corner_pass(p).start)

    per = r.got.shape[1] * r.got.shape[2]
    ff = r.wg.shape[2]
    coefs = [None] * 4

    def serve_up(p):
        g = groups[p]
        shape = (r.got.shape[1], tok, LANES)
        lanes = lax.broadcasted_iota(jnp.int32, shape, 2)
        chosen = lanes == lax.broadcasted_iota(jnp.int32, shape, 1)
        rates = jnp.where(chosen, jnp.broadcast_to(r.rates[g, :, sp], shape), 0.0)
        coefs[p] = jnp.sum(rates.reshape(per, LANES), axis=1, keepdims=True)

        @pl.loop(0, PAIR)
        def _(i):
            rows = r.got[g].reshape(per, width)
            gate = jnp.dot(rows, r.wg[i], preferred_element_type=jnp.float32)
            up = jnp.dot(rows, r.wu[i], preferred_element_type=jnp.float32)
            gate = jnp.minimum(gate, clamp_limit)
            up = jnp.clip(up, -clamp_limit, clamp_limit)
            r.active[i] = narrow(gate * jax.nn.sigmoid(swish_alpha * gate) * (up + 1.0))

    def serve_down(p):
        step = min(width, 1024)

        @pl.loop(0, width // step)
        def _(i):
            cols = pl.ds(pl.multiple_of(i * step, step), step)
            down = jnp.dot(r.active[0], r.wd[0, :, cols], preferred_element_type=jnp.float32)
            for j in range(1, PAIR):
                down = down + jnp.dot(
                    r.active[j], r.wd[j, :, cols], preferred_element_type=jnp.float32
                )
            r.summed[p, :, :, cols] = narrow(down * coefs[p]).reshape(
                r.summed.shape[1:3] + (step,)
            )

    dx_copy, dy_copy = [None] * 4, [None] * 4
    bx_copy, by_copy = [[] for _ in range(4)], [[] for _ in range(4)]
    home = [None] * 4

    def give_x(p, i, rows):
        bx_copy[p].append(
            send(
                r.summed.at[p, xb, rows], r.x_in.at[p, rows],
                r.bx_s.at[p, i], r.bx_r.at[p, i], to_x,
            )
        )

    def give_y(p, i, rows):
        by_copy[p].append(
            send(
                r.summed.at[p, yb, rows], r.y_in.at[p, rows],
                r.by_s.at[p, i], r.by_r.at[p, i], to_y,
            )
        )

    def corner_home(p):
        return remote(
            r.summed.at[p, db], r.corner_in.at[z], r.e_s.at[p], r.e_r.at[z], to_z[p]
        )

    def fold(p):
        if p == 0:
            give_x(p, 0, top)
            give_y(p, 0, bottom)
        elif p in through:
            halves(p)
            give_x(p, 0, top)
            give_y(p, 0, bottom)
        else:
            started.append(corner_home(p))
            started[-1].start()
            give_x(p, 0, slice(None))
            give_y(p, 0, slice(None))

    def halves(p):
        dx_copy[p] = send(
            r.summed.at[p, db, top], r.dx_in.at[p], r.dx_s.at[p], r.dx_r.at[p], to_x
        )
        dy_copy[p] = send(
            r.summed.at[p, db, bottom], r.dy_in.at[p], r.dy_s.at[p], r.dy_r.at[p], to_y
        )

    def feed():
        def take(p):
            g = groups[p]
            remote(
                r.summed.at[p, db], r.corner_in.at[g], r.e_s.at[p], r.e_r.at[g], to_z[p]
            ).wait_recv()
            return wide(r.corner_in[g])

        @pl.when(inner)
        def _():
            r.summed[0, db] = narrow(wide(r.summed[0, db]) + take(1) + take(2) + take(3))

        @pl.when(outer)
        def _():
            r.summed[0, db] = narrow(wide(r.summed[0, db]) + take(1))

        halves(0)

    def join(p):
        dx_copy[p].wait_recv()
        r.summed[p, yb, top] = narrow(wide(r.summed[p, yb, top]) + wide(r.dx_in[p]))
        give_y(p, 1, top)
        dy_copy[p].wait_recv()
        r.summed[p, xb, bottom] = narrow(wide(r.summed[p, xb, bottom]) + wide(r.dy_in[p]))
        give_x(p, 1, bottom)

    def gather(p):
        for copy in bx_copy[p] + by_copy[p]:
            copy.wait_recv()
        return wide(r.summed[p, mine]) + wide(r.x_in[p]) + wide(r.y_in[p])

    def leave(p):
        r.home_out[p] = narrow(gather(p))
        home[p] = send(
            r.home_out.at[p], r.home_in.at[z], r.b_s.at[p], r.b_r.at[z], to_z[p]
        )

    def corner_out():
        corner_z(0).start()
        pl.when(inner)(corner_pass(0).start)

    def on_inner(action, *args):
        pl.when(inner)(functools.partial(action, *args))

    def on_outer(action, *args):
        pl.when(outer)(functools.partial(action, *args))

    with jax.named_scope("spread"):
        begin()
        cross_first(0)
        spread(1, 0)
        on_inner(spread, 2, 0)
        cross_rest(0)
        spread(1, 1)
        on_inner(spread, 2, 1)
        corner(0)
        on_outer(corner_out)
        on_inner(spread, 3, 0)
        on_inner(spread, 3, 1)
        on_inner(corner_out)
        on_outer(spread, 2, 0)
        on_outer(spread, 2, 1)
    for copy in shared:
        copy.wait_recv()
    for copy in rates_y:
        copy.wait_recv()
    with jax.named_scope("serve"):
        serve_up(0)
        serve_down(0)
        on_outer(spread, 3, 0)
        on_outer(spread, 3, 1)
        fold(0)
        cross_rest(1)
        corner(1)
        cross_first(3)
        serve_up(1)
        serve_down(1)
        fold(1)
        cross_rest(2)
        corner(2)
        serve_up(2)
        serve_down(2)
        fold(2)
        cross_rest(3)
        corner(3)
        serve_up(3)
        serve_down(3)
        fold(3)
        leave(1)
        leave(2)
        join(3)
        feed()
        leave(3)
        join(0)

        def arrived(p):
            g = groups[p]
            remote(
                r.home_out.at[p], r.home_in.at[g], r.b_s.at[p], r.b_r.at[g], to_z[p]
            ).wait_recv()
            return wide(r.home_in[g])

        near = arrived(1) + arrived(2)
        mixture = near + gather(0)
    with jax.named_scope("back"):
        mixture = mixture + arrived(3)
        r.out[...] = (r.middle[...] + scale_rows(mixture, r.gain_moe[...])).astype(r.out.dtype)
        for copy in started:
            copy.wait_send()

        @pl.when(inner)
        def _():
            for copy in inner_started:
                copy.wait_send()


def whole_layer(
    queries, keys, values, q_gain, k_gain, w_out, residual, gain_mix, gain_pre, routes,
    route_weights, w_gate, w_up, w_down, gain_moe,
):
    tokens, heads, size = queries.shape
    kv_cols = keys.shape[1] * size
    tok, width = residual.shape
    ff = w_gate.shape[1]
    blocks = PAIR * PAIR
    half = tok // 2
    pieces = 4
    bf, f32 = jnp.bfloat16, jnp.float32
    dma = pltpu.SemaphoreType.DMA
    here = pl.BlockSpec(memory_space=pltpu.VMEM)
    there = pl.BlockSpec(memory_space=pl.ANY)
    scratch = {
        "kv": pltpu.VMEM((2, RING, PAIR, tokens, kv_cols), bf),
        "query": pltpu.VMEM((tokens * heads, kv_cols), bf),
        "top": pltpu.VMEM((tokens * heads, size), f32),
        "total": pltpu.VMEM((tokens * heads, size), f32),
        "mixed": pltpu.VMEM((tokens * heads, size), f32),
        "heads": pltpu.VMEM((tokens, heads * size), bf),
        "wo": pltpu.VMEM((heads * size, width), bf),
        "part": pltpu.VMEM((PAIR, PAIR, tok, width), bf),
        "wg": pltpu.VMEM((PAIR, width, ff), bf),
        "wu": pltpu.VMEM((PAIR, width, ff), bf),
        "wd": pltpu.VMEM((PAIR, ff, width), bf),
        "pc_in": pltpu.VMEM((PAIR, tok, width), bf),
        "py_out": pltpu.VMEM((tok, width), bf),
        "py_in": pltpu.VMEM((tok, width), bf),
        "got": pltpu.VMEM((RING, blocks, tok, width), bf),
        "rates": pltpu.VMEM((RING, blocks, RING * PAIR, 1, LANES), f32),
        "middle": pltpu.VMEM((tok, width), f32),
        "active": pltpu.VMEM((PAIR, blocks * tok, ff), bf),
        "summed": pltpu.VMEM((RING, blocks, tok, width), bf),
        "dx_in": pltpu.VMEM((RING, half, width), bf),
        "dy_in": pltpu.VMEM((RING, half, width), bf),
        "x_in": pltpu.VMEM((RING, tok, width), bf),
        "corner_in": pltpu.VMEM((RING, tok, width), bf),
        "y_in": pltpu.VMEM((RING, tok, width), bf),
        "home_out": pltpu.VMEM((RING, tok, width), bf),
        "home_in": pltpu.VMEM((RING, tok, width), bf),
        "queries": pltpu.VMEM(queries.shape, bf),
        "residual": pltpu.VMEM(residual.shape, bf),
        "gain_mix": pltpu.VMEM(gain_mix.shape, f32),
        "gain_pre": pltpu.VMEM(gain_pre.shape, f32),
        "gain_moe": pltpu.VMEM(gain_moe.shape, f32),
        "q_sem": dma((5,)),
        "w_sem": dma((4,)),
    }
    for name, dims in (
        ("kz", (4, 2)), ("kx", (4, 2)), ("kf", (4, 2)), ("pc", (pieces,)), ("py", (pieces,)), ("z", (4, 2)), ("x", (4, 2)), ("y", (4, 2)), ("zf", (4, 2)), ("d", (4,)), ("df", (4,)), ("e", (4,)), ("hx", (4,)),
        ("hy", (4,)), ("w", (3,)), ("az", (4,)), ("ax", (1,)), ("ay", (2,)), ("dx", (4,)), ("dy", (4,)), ("bx", (4, 2)),
        ("by", (4, 2)), ("b", (4,)),
    ):
        scratch[name + "_s"] = dma(dims)
        scratch[name + "_r"] = dma(dims)
    operands = (
        "keys", "values", "q_gain", "k_gain", "routes", "route_weights", "queries_hbm",
        "residual_hbm", "mix_hbm", "pre_hbm", "moe_hbm", "wo_hbm", "wg_hbm", "wu_hbm", "wd_hbm",
    )
    names = operands + ("out",) + tuple(scratch)
    return pl.pallas_call(
        functools.partial(layer_kernel, names),
        out_shape=jax.ShapeDtypeStruct((tok, width), bf),
        in_specs=[here] * 6 + [there] * 9,
        out_specs=here,
        scratch_shapes=list(scratch.values()),
        compiler_params=pltpu.CompilerParams(
            collective_id=1, has_side_effects=True, vmem_limit_bytes=56 << 20
        ),
        name="whole_layer",
    )(
        keys, values, q_gain, k_gain, routes, route_weights, queries, residual, gain_mix,
        gain_pre, gain_moe, w_out, w_gate, w_up, w_down,
    )


def on_device(
    queries,
    keys,
    values,
    q_gain,
    k_gain,
    w_out,
    residual,
    gain_mix,
    gain_pre,
    routes,
    route_weights,
    w_gate,
    w_up,
    w_down,
    gain_moe,
):
    local_experts = w_gate.shape[0]
    experts_all = local_experts * lax.axis_size("sp")
    tok_part, width = residual.shape
    capacity = max(2, (2 * tok_part * TOP + experts_all - 1) // experts_all)
    grid_fits = lax.axis_size("sp") == RING * PAIR and lax.axis_size("tp") == PAIR * PAIR
    if grid_fits and local_experts == 1 and capacity >= tok_part:
        return whole_layer(
            queries, keys, values, q_gain[None], k_gain[None], w_out, residual,
            gain_mix[None], gain_pre[None], routes.T, route_weights.T, w_gate[0], w_up[0],
            w_down[0], gain_moe[None],
        )
    tok_rows, head_local, head_size = queries.shape
    kv_local = keys.shape[1]
    group_size = head_local // kv_local
    positions = lax.axis_index("sp") * tok_rows + jnp.arange(tok_rows, dtype=jnp.int32)
    cosine_table, sine_table = rope_tables(positions, head_size)
    q_turned = (
        turn(scale_rows(queries.astype(jnp.float32), q_gain), cosine_table, sine_table)
        * head_size ** (-0.5)
    ).astype(jnp.bfloat16)
    k_turned = turn(scale_rows(keys.astype(jnp.float32), k_gain), cosine_table, sine_table).astype(
        jnp.bfloat16
    )
    q_grouped = q_turned.reshape(tok_rows, kv_local, group_size, head_size)
    initial = (
        jnp.full((kv_local, group_size, tok_rows), -jnp.inf, jnp.float32),
        jnp.zeros((kv_local, group_size, tok_rows), jnp.float32),
        jnp.zeros((kv_local, group_size, tok_rows, head_size), jnp.float32),
    )
    carry_state = initial
    kv_cols = kv_local * head_size
    both = gather_sp(
        jnp.concatenate(
            [k_turned.reshape(tok_rows, kv_cols), values.reshape(tok_rows, kv_cols)], axis=1
        )
    ).reshape(-1, 2 * kv_cols)
    key_piece = both[:, :kv_cols].reshape(-1, kv_local, head_size)
    value_piece = both[:, kv_cols:].reshape(-1, kv_local, head_size)
    piece_rows = key_piece.shape[0]
    block_rows = math.gcd(piece_rows, 1024)
    key_blocks = key_piece.reshape(piece_rows // block_rows, block_rows, kv_local, head_size)
    value_blocks = value_piece.reshape(piece_rows // block_rows, block_rows, kv_local, head_size)

    def absorb_block(state_now, key_value):
        running_max, running_sum, weighted = state_now
        key_block, value_block = key_value
        scores = jnp.einsum(
            "qkgd,skd->kgqs", q_grouped, key_block, preferred_element_type=jnp.float32
        )
        new_max = jnp.maximum(running_max, jnp.max(scores, axis=-1))
        rescale = jnp.exp(running_max - new_max)
        unnorm = jnp.exp(scores - new_max[..., None])
        running_sum = running_sum * rescale + jnp.sum(unnorm, axis=-1)
        weighted = weighted * rescale[..., None] + jnp.einsum(
            "kgqs,skd->kgqd",
            unnorm.astype(jnp.bfloat16),
            value_block,
            preferred_element_type=jnp.float32,
        )
        return ((new_max, running_sum, weighted), None)

    carry_state, ignored = lax.scan(absorb_block, carry_state, (key_blocks, value_blocks))
    running_max, running_sum, weighted = carry_state
    mixed_heads = (weighted / running_sum[..., None]).transpose(2, 0, 1, 3)
    mixed_heads = mixed_heads.reshape(tok_rows, head_local * head_size).astype(jnp.bfloat16)
    part = jnp.dot(mixed_heads, w_out, preferred_element_type=jnp.float32).astype(jnp.bfloat16)
    projected = lax.psum_scatter(
        part,
        "tp",
        scatter_dimension=0,
        tiled=True,
    ).astype(jnp.float32)
    middle = residual.astype(jnp.float32) + scale_rows(projected, gain_mix)
    normed = scale_rows(middle, gain_pre).astype(jnp.bfloat16)
    tables = slot_table(routes, experts_all, capacity)
    chosen = jnp.sum(tables, axis=1)
    outbound = jnp.einsum("tp,td->pd", chosen, normed, preferred_element_type=jnp.float32)
    outbound = outbound.astype(jnp.bfloat16).reshape(experts_all, capacity, width)
    arrived_rows = lax.all_gather(
        lax.all_to_all(outbound, "sp", split_axis=0, concat_axis=0, tiled=True),
        "tp",
        axis=0,
        tiled=True,
    )
    leading = arrived_rows.shape[0] // local_experts
    partial_value = expert_apply(
        arrived_rows.reshape(leading, local_experts, arrived_rows.shape[1], width),
        w_gate,
        w_up,
        w_down,
    )
    summed = lax.psum_scatter(
        partial_value.reshape(arrived_rows.shape).astype(jnp.bfloat16),
        "tp",
        scatter_dimension=0,
        tiled=True,
    )
    returned = send_back(summed)
    gathered = jnp.einsum(
        "tkp,pd->tkd",
        tables,
        returned.reshape(experts_all * capacity, width),
        preferred_element_type=jnp.float32,
    )
    mixture = jnp.sum(gathered * route_weights[:, :, None], axis=1)
    return (middle + scale_rows(mixture, gain_moe)).astype(jnp.bfloat16)


def solution(mesh):
    placed = (
        P("sp", "tp", None),
        P("sp", "tp", None),
        P("sp", "tp", None),
        P(),
        P(),
        P("tp", None),
        P(("sp", "tp"), None),
        P(),
        P(),
        P(("sp", "tp"), None),
        P(("sp", "tp"), None),
        P("sp", None, "tp"),
        P("sp", None, "tp"),
        P("sp", "tp", None),
        P(),
    )
    return jax.shard_map(
        on_device, mesh=mesh, in_specs=placed, out_specs=P(("sp", "tp"), None), check_vma=False
    )
```
